256 devices in a mesh: ra: 16 (over y, x), cb: 16 (over z, core).
Axes of the slice: x: 4, y: 4, z: 8, core: 2. Of those that a mesh axis runs over, the one named last changes fastest.
Arguments:
- tokens: bfloat16 [768, 4096], P(None, 'ra'), may hold values from -27 to 27, as said below
- gain_first: float32 [4096], P('ra'), may hold values from 0.1 to 1.9
- up_first: bfloat16 [4096, 16384], P('ra', 'cb'), may hold values from -0.09375 to 0.09375
- down_first: bfloat16 [16384, 4096], P('cb', 'ra'), may hold values from -0.046875 to 0.046875
- gain_second: float32 [4096], P('ra'), may hold values from 0.1 to 1.9
- up_second: bfloat16 [4096, 16384], P('ra', 'cb'), may hold values from -0.09375 to 0.09375
- down_second: bfloat16 [16384, 4096], P('cb', 'ra'), may hold values from -0.046875 to 0.046875
Outputs:
- mixed: bfloat16 [768, 4096], P(None, 'ra')
The draws below stay inside these ranges and needn't reach their ends.
Inputs may be any that keep to these rules, and one draw needn't show every extreme that they name: `tokens`: channels come in 32 groups of equal width with different scales.
All inputs are finite; a program needn't handle non-finite values.
Results may differ from the reference program's by a relative error of at most 0.0079.
Values may be sent and summed in bfloat16 or wider, within the bound.
No kernel may reach another device: no remote copies, remote signals or barrier semaphores. Data moves between devices by JAX's collectives and lax.ppermute only.
A program may use at most 64 MiB of HBM per device.

```python
import jax
import jax.numpy as jnp
from jax import lax

D = 4096
FF = 16384
TOK = 768


def draw_tokens(key, part):
    key_base = jax.random.fold_in(key, 11)
    key_group = jax.random.fold_in(key, 12)
    base = jnp.clip(jax.random.normal(key_base, (TOK, D), jnp.float32), -4.0, 4.0)
    groups = jnp.exp(jax.random.uniform(key_group, (32,), jnp.float32, -1.2, 1.2))
    channel = jnp.repeat(groups, D // 32)
    return (base * channel[None, :]).astype(jnp.bfloat16)


def shard_levels(rng, extent, split, least, largest):
    def one(dim, blocks):
        heights = jax.random.uniform(jax.random.fold_in(jax.random.fold_in(rng, 6), dim), (blocks,), jnp.float32, least / len(split), largest / len(split))
        return jnp.repeat(jnp.exp(heights), extent[dim] // blocks).reshape((-1,) + (1,) * (len(extent) - dim - 1))

    factor_of = one(*split[0])
    for cut in split[1:]:
        factor_of = factor_of * one(*cut)
    return factor_of


def noise(key, extent, deviation, bound, shards=(), kind=jnp.bfloat16):
    factor_of = shard_levels(key, extent, shards, -0.22, 0.18) if shards else 1.0
    array = jax.random.normal(key, extent, jnp.float32) * deviation * factor_of
    return jnp.minimum(jnp.maximum(array, -bound), bound).astype(kind)


def setup_inputs(seed: int = 0) -> dict:
    seeds = jax.random.split(jax.random.key(seed), 8)
    return {
        "tokens": draw_tokens(jax.random.fold_in(seeds[7], 71), 0),
        "gain_first": jnp.clip(1.0 + 0.18 * jax.random.normal(seeds[1], (D,), jnp.float32), 0.1, 1.9),
        "up_first": noise(seeds[2], (D, FF), D ** -0.5, 0.09375, ((0, 16), (1, 16))),
        "down_first": noise(seeds[3], (FF, D), FF ** -0.5, 0.046875, ((0, 16), (1, 16))),
        "gain_second": jnp.clip(1.0 + 0.18 * jax.random.normal(seeds[4], (D,), jnp.float32), 0.1, 1.9),
        "up_second": noise(seeds[5], (D, FF), D ** -0.5, 0.09375, ((0, 16), (1, 16))),
        "down_second": noise(seeds[6], (FF, D), FF ** -0.5, 0.046875, ((0, 16), (1, 16))),
    }


def sublayer(x, gain, w_up, w_down):
    xf = x.astype(jnp.float32)
    meansq = lax.optimization_barrier(jnp.mean(xf * xf, axis=1))
    scaled = (xf * gain.astype(jnp.float32)[None, :]).astype(jnp.bfloat16)
    pre = jnp.dot(scaled, w_up, preferred_element_type=jnp.float32)
    act = jax.nn.relu(pre * jax.lax.rsqrt(meansq + 1e-06)[:, None])
    hidden = (act * act).astype(jnp.bfloat16)
    branch = jnp.dot(hidden, w_down, preferred_element_type=jnp.float32)
    return (0.5 * xf + branch).astype(jnp.bfloat16)

def reference(tokens, gain_first, up_first, down_first, gain_second, up_second, down_second):
    middle = sublayer(tokens, gain_first, up_first, down_first)
    return sublayer(middle, gain_second, up_second, down_second)
```

```python
import jax
import jax.numpy as jnp
from jax import lax
from jax.sharding import Mesh, PartitionSpec as P

RA = ("y", "x")
BF = jnp.bfloat16
F32 = jnp.float32


def exchange(parts, axis):
    return lax.all_to_all(parts, axis, 0, 0, tiled=True)


def copy_for_each(x, axis):
    peers = lax.axis_size(axis)
    return exchange(jnp.broadcast_to(x[None], (peers, *x.shape)), axis)


def from_other_core(w):
    return lax.ppermute(w, "c", [(0, 1), (1, 0)])


def sublayer(x, gain, up_own, up_other, down_own, down_other, width):
    tokens, _ = x.shape
    peers = lax.axis_size(RA)
    xf = x.astype(F32)
    sq = jnp.sum(xf * xf, axis=1, keepdims=True)
    high = sq.astype(BF)
    low = (sq - high.astype(F32)).astype(BF)
    scaled = (xf * gain[None, :]).astype(BF)
    up = jnp.concatenate([up_own, up_other], axis=1)
    hidden_width = up.shape[1]
    pre = jnp.dot(scaled, up, preferred_element_type=F32).astype(BF)
    stats = jnp.concatenate([high, low, jnp.zeros((tokens, 126), BF)], axis=1)
    payload = jnp.concatenate([pre, stats], axis=1).reshape(peers, tokens // peers, -1)
    total = jnp.sum(exchange(payload, RA).astype(F32), axis=0)
    meansq = (total[:, hidden_width] + total[:, hidden_width + 1]) / width
    act = jax.nn.relu(total[:, :hidden_width] * lax.rsqrt(meansq + 1e-06)[:, None])
    hidden = copy_for_each((act * act).astype(BF), RA).reshape(tokens, hidden_width)
    down = jnp.concatenate([down_own, down_other], axis=0)
    branch = jnp.dot(hidden, down, preferred_element_type=F32).astype(BF)
    planes = lax.axis_size("z")
    count = tokens // planes
    rows = jnp.sum(exchange(branch.reshape(planes, count, -1), "z").astype(F32), axis=0)
    own = lax.dynamic_slice_in_dim(xf, lax.axis_index("z") * count, count, 0)
    finished = (0.5 * own + rows).astype(BF)
    return copy_for_each(finished, "z").reshape(tokens, -1)


def body(tokens, gain_first, up_first, down_first, gain_second, up_second, down_second):
    width = tokens.shape[1] * lax.axis_size(RA)
    half = tokens.shape[0] // 2
    core = lax.axis_index("c")
    x = lax.dynamic_slice_in_dim(tokens, core * half, half, 0)
    others = [from_other_core(w) for w in (up_first, down_first, up_second, down_second)]
    x = sublayer(x, gain_first, up_first, others[0], down_first, others[1], width)
    x = sublayer(x, gain_second, up_second, others[2], down_second, others[3], width)
    y = from_other_core(x)
    first = core == 0
    return jnp.concatenate([jnp.where(first, x, y), jnp.where(first, y, x)], axis=0)


def solution(mesh):
    fine = Mesh(mesh.devices.reshape(4, 4, 8, 2), ("y", "x", "z", "c"))
    cb = ("z", "c")
    placed = (
        P(None, RA),
        P(RA),
        P(RA, cb),
        P(cb, RA),
        P(RA),
        P(RA, cb),
        P(cb, RA),
    )
    return jax.shard_map(body, mesh=fine, in_specs=placed, out_specs=P(None, RA), check_vma=False)
```

```python
import functools

import jax
import jax.numpy as jnp
from jax import lax
from jax.experimental import pallas as pl
from jax.experimental.pallas import tpu as pltpu
from jax.sharding import Mesh, PartitionSpec as P

RA = ("y", "x")
BF = jnp.bfloat16
F32 = jnp.float32
LANES = 128
EPS = 1e-06


def exchange(parts, axis):
    return lax.all_to_all(parts, axis, 0, 0, tiled=True)


def from_other_core(w):
    return lax.ppermute(w, "c", [(0, 1), (1, 0)])


def along_y(a, shift):
    n = lax.axis_size("y")
    return lax.ppermute(a, "y", [(i, (i + shift) % n) for i in range(n)])


def by_plane(a, sign):
    ny, nz = lax.axis_size("y"), lax.axis_size("z")
    perm = [(y * nz + z, (y + sign * (z // 2)) % ny * nz + z) for y in range(ny) for z in range(nz)]
    return lax.ppermute(a, ("y", "z"), perm)


def call(kernel, out, scratch=(), limit=16):
    vmem = pl.BlockSpec(memory_space=pltpu.VMEM)

    def run(*args):
        return pl.pallas_call(
            kernel,
            out_shape=out,
            in_specs=[vmem] * len(args),
            out_specs=jax.tree.map(lambda _: vmem, out),
            scratch_shapes=list(scratch),
            compiler_params=pltpu.CompilerParams(vmem_limit_bytes=limit << 20),
        )(*args)

    return run


def sds(shape, dtype=BF):
    return jax.ShapeDtypeStruct(shape, dtype)


def stat_columns(sq):
    high = sq.astype(BF)
    low = (sq - high.astype(F32)).astype(BF)
    lane = lax.broadcasted_iota(jnp.int32, (sq.shape[0], LANES), 1)
    block = jnp.where(lane == 0, high.astype(F32), jnp.where(lane == 1, low.astype(F32), 0.0))
    return block.astype(BF)


def up_first_kernel(tokens, gain, own, other, out):
    half, hid = tokens.shape[0] // 2, own.shape[1]
    start = pl.multiple_of(lax.axis_index("c") * half, half)
    xf = tokens[pl.ds(start, half), :].astype(F32)
    scaled = (xf * gain[...]).astype(BF)
    out[:, :hid] = jnp.dot(scaled, own[...], preferred_element_type=F32).astype(BF)
    out[:, hid : 2 * hid] = jnp.dot(scaled, other[...], preferred_element_type=F32).astype(BF)
    out[:, 2 * hid :] = stat_columns(jnp.sum(xf * xf, axis=1, keepdims=True))


def down_first_kernel(hidden, *refs):
    out = refs[-1]
    n = (len(refs) - 1) // 2
    k = refs[0].shape[0]
    for d in range(n):
        acc = jnp.dot(hidden[:, :k], refs[d][...], preferred_element_type=F32)
        acc += jnp.dot(hidden[:, k:], refs[n + d][...], preferred_element_type=F32)
        acc = acc.astype(BF)
        out[2 * d] = acc[:, :LANES]
        out[2 * d + 1] = acc[:, LANES:]


def finish_first_kernel(parts, kept, mid, payload):
    rows = mid.shape[0]
    total = parts[0].astype(F32)
    for i in range(1, parts.shape[0]):
        total += parts[i].astype(F32)
    x = (0.5 * kept[:rows, :] + total).astype(BF)
    gain = kept[rows:, :]
    high = gain.astype(BF).astype(F32)
    rest = gain - high
    middle = rest.astype(BF).astype(F32)
    low = rest - middle
    row = lax.broadcasted_iota(jnp.int32, gain.shape, 0)
    coded = jnp.where(row == 0, high, jnp.where(row == 1, middle, low)).astype(BF)
    mid[...] = x
    for i in range(payload.shape[0]):
        payload[i, :rows, :] = x
        payload[i, rows:, :] = coded


def up_second_kernel(x, *refs):
    out = refs[-1]
    n = (len(refs) - 1) // 2
    hid = refs[0].shape[1]
    rows = out.shape[0]
    scaled, sq = [], jnp.zeros((rows, 1), F32)
    for i in range(x.shape[0]):
        xf = x[i, :rows, :].astype(F32)
        coded = x[i, rows:, :].astype(F32)
        gain = coded[0:1] + coded[1:2] + coded[2:3]
        sq += jnp.sum(xf * xf, axis=1, keepdims=True)
        scaled.append((xf * gain).astype(BF))
    scaled = jnp.concatenate(scaled, axis=1)
    depth = refs[0].shape[0]
    for side in range(2):
        acc = jnp.zeros((rows, hid), F32)
        for d in range(n):
            acc += jnp.dot(
                scaled[:, d * depth : (d + 1) * depth], refs[side * n + d][...], preferred_element_type=F32
            )
        out[:, side * hid : (side + 1) * hid] = acc.astype(BF)
    out[:, 2 * hid :] = stat_columns(sq)


def down_second_kernel(hidden, own, other, out, acc):
    k = own.shape[0]
    n, rows, _ = acc.shape
    total = jnp.dot(hidden[:, :k], own[...], preferred_element_type=F32)
    total += jnp.dot(hidden[:, k:], other[...], preferred_element_type=F32)
    for i in range(n):
        acc[i] = total[i * rows : (i + 1) * rows]
    y = lax.axis_index("y")
    for d in range(n):
        block = acc[lax.rem(y + d, n)].astype(BF)
        out[2 * d] = block[:, :LANES]
        out[2 * d + 1] = block[:, LANES:]


def finish_second_kernel(parts, kept, payload):
    total = parts[0].astype(F32)
    for i in range(1, parts.shape[0]):
        total += parts[i].astype(F32)
    x = (0.5 * kept[...].astype(F32) + total).astype(BF)
    for i in range(payload.shape[0]):
        payload[i] = x


def assemble_kernel(own, other, out):
    chunks, rows, _ = own.shape
    n = chunks // 2
    y, c = lax.axis_index("y"), lax.axis_index("c")
    for side, ref in ((c, own), (1 - c, other)):
        for d in range(n):
            start = pl.multiple_of((side * n + lax.rem(y + d, n)) * rows, rows)
            out[pl.ds(start, rows), :LANES] = ref[2 * d]
            out[pl.ds(start, rows), LANES:] = ref[2 * d + 1]


def activate(parts, hid, width):
    total = jnp.sum(parts.astype(F32), axis=0)
    meansq = (total[:, hid : hid + 1] + total[:, hid + 1 : hid + 2]) / width
    act = jax.nn.relu(total[:, :hid] * lax.rsqrt(meansq + EPS))
    return (act * act).astype(BF)


def spread(x, peers):
    return jnp.broadcast_to(x[None], (peers, *x.shape))


def body(tokens, gain_first, up_first, down_first, gain_second, up_second, down_second):
    ny, nx, nz = lax.axis_size("y"), lax.axis_size("x"), lax.axis_size("z")
    y, z, c = lax.axis_index("y"), lax.axis_index("z"), lax.axis_index("c")
    count, channels = tokens.shape
    width = channels * ny * nx
    half = count // 2
    per_y = half // ny
    few = per_y // nx
    hid = 2 * up_first.shape[1]

    payload = call(up_first_kernel, sds((half, hid + LANES)))(
        tokens, gain_first[None, :], up_first, from_other_core(up_first)
    )
    parts = exchange(payload.reshape(ny * nx, few, hid + LANES), RA)

    downs = [down_first] + [along_y(down_first, d) for d in range(1, ny)]
    ups = [up_second] + [along_y(up_second, d) for d in range(1, ny)]
    other_downs = [from_other_core(w) for w in downs]
    other_ups = [from_other_core(w) for w in ups]
    other_last = from_other_core(down_second)

    start = c * half + lax.rem(y + z // 2, ny) * per_y
    column = lax.rem(z, 2) * LANES
    kept = lax.dynamic_slice(tokens, (start, column), (per_y, LANES)).astype(F32)
    gain = lax.dynamic_slice(gain_second, (column,), (LANES,))
    kept = by_plane(jnp.concatenate([kept, jnp.broadcast_to(gain[None], (8, LANES))], axis=0), 1)

    hidden = activate(parts, hid, width)
    hidden = exchange(spread(hidden, nx), "x").reshape(per_y, hid)
    branch = call(down_first_kernel, sds((nz, per_y, LANES)))(hidden, *downs, *other_downs)
    middle, payload = call(finish_first_kernel, (sds((per_y, LANES)), sds((nz, per_y + 8, LANES))))(
        exchange(branch, "z"), kept
    )
    middle = by_plane(middle, -1)
    payload = call(up_second_kernel, sds((per_y, hid + LANES)))(exchange(payload, "z"), *ups, *other_ups)
    hidden = activate(exchange(payload.reshape(nx, few, hid + LANES), "x"), hid, width)
    hidden = exchange(spread(hidden, ny * nx), RA).reshape(half, hid)
    branch = call(
        down_second_kernel, sds((nz, per_y, LANES)), [pltpu.VMEM((ny, per_y, channels), F32)]
    )(hidden, down_second, other_last)
    payload = call(finish_second_kernel, sds((nz, per_y, LANES)))(exchange(branch, "z"), middle)
    rows = exchange(payload, "z")
    return call(assemble_kernel, sds((count, channels)))(rows, from_other_core(rows))


def solution(mesh):
    fine = Mesh(mesh.devices.reshape(4, 4, 8, 2), ("y", "x", "z", "c"))
    cb = ("z", "c")
    placed = (
        P(None, RA),
        P(RA),
        P(RA, cb),
        P(cb, RA),
        P(RA),
        P(RA, cb),
        P(cb, RA),
    )
    return jax.shard_map(body, mesh=fine, in_specs=placed, out_specs=P(None, RA), check_vma=False)
```

```python
import functools

import jax
import jax.numpy as jnp
from jax import lax
from jax.experimental import pallas as pl
from jax.experimental.pallas import tpu as pltpu
from jax.sharding import Mesh, PartitionSpec as P

RA = ("y", "x")
BF = jnp.bfloat16
F32 = jnp.float32
LANES = 128
EPS = 1e-06


def exchange(parts, axis):
    return lax.all_to_all(parts, axis, 0, 0, tiled=True)


def from_other_core(w):
    return lax.ppermute(w, "c", [(0, 1), (1, 0)])


def along_y(a, shift):
    n = lax.axis_size("y")
    return lax.ppermute(a, "y", [(i, (i + shift) % n) for i in range(n)])


def by_plane(a, sign):
    ny, nz = lax.axis_size("y"), lax.axis_size("z")
    perm = [(y * nz + z, (y + sign * (z // 2)) % ny * nz + z) for y in range(ny) for z in range(nz)]
    return lax.ppermute(a, ("y", "z"), perm)


def call(kernel, out, scratch=(), limit=16):
    vmem = pl.BlockSpec(memory_space=pltpu.VMEM)

    def run(*args):
        return pl.pallas_call(
            kernel,
            out_shape=out,
            in_specs=[vmem] * len(args),
            out_specs=jax.tree.map(lambda _: vmem, out),
            scratch_shapes=list(scratch),
            compiler_params=pltpu.CompilerParams(vmem_limit_bytes=limit << 20),
        )(*args)

    return run


def sds(shape, dtype=BF):
    return jax.ShapeDtypeStruct(shape, dtype)


def stat_columns(sq):
    high = sq.astype(BF)
    low = (sq - high.astype(F32)).astype(BF)
    lane = lax.broadcasted_iota(jnp.int32, (sq.shape[0], LANES), 1)
    block = jnp.where(lane == 0, high.astype(F32), jnp.where(lane == 1, low.astype(F32), 0.0))
    return block.astype(BF)


def up_first_kernel(tokens, gain, own, other, out, *, ny, nx):
    half, hid = tokens.shape[0] // 2, own.shape[1]
    start = pl.multiple_of(lax.axis_index("c") * half, half)
    xf = tokens[pl.ds(start, half), :].astype(F32)
    few = half // (ny * nx)
    order = [(y * nx + x) * few for x in range(nx) for y in range(ny)]
    xf = jnp.concatenate([xf[i : i + few] for i in order], axis=0)
    scaled = (xf * gain[...]).astype(BF)
    out[:, :hid] = jnp.dot(scaled, own[...], preferred_element_type=F32).astype(BF)
    out[:, hid : 2 * hid] = jnp.dot(scaled, other[...], preferred_element_type=F32).astype(BF)
    out[:, 2 * hid :] = stat_columns(jnp.sum(xf * xf, axis=1, keepdims=True))


def summed(parts):
    total = parts[0].astype(F32)
    for i in range(1, parts.shape[0]):
        total += parts[i].astype(F32)
    return total


def pass_on_kernel(parts, out):
    hid = parts.shape[2] - LANES
    total = summed(parts)
    out[:, :hid] = total[:, :hid].astype(BF)
    out[:, hid:] = stat_columns(total[:, hid : hid + 1] + total[:, hid + 1 : hid + 2])


def activate_kernel(parts, out, *, width):
    hid = parts.shape[2] - LANES
    total = summed(parts)
    meansq = (total[:, hid : hid + 1] + total[:, hid + 1 : hid + 2]) / width
    act = jnp.maximum(total[:, :hid] * lax.rsqrt(meansq + EPS), 0.0)
    act = (act * act).astype(BF)
    for i in range(out.shape[0]):
        out[i] = act


def down_kernel(hidden, *refs):
    out = refs[-1]
    n = (len(refs) - 1) // 2
    k = refs[0].shape[0]
    for d in range(n):
        acc = jnp.dot(hidden[:, :k], refs[d][...], preferred_element_type=F32)
        acc += jnp.dot(hidden[:, k:], refs[n + d][...], preferred_element_type=F32)
        acc = acc.astype(BF)
        out[2 * d] = acc[:, :LANES]
        out[2 * d + 1] = acc[:, LANES:]


def finish_first_kernel(parts, kept, mid, payload):
    rows = mid.shape[0]
    x = (0.5 * kept[:rows, :] + summed(parts)).astype(BF)
    gain = kept[rows:, :]
    high = gain.astype(BF).astype(F32)
    rest = gain - high
    middle = rest.astype(BF).astype(F32)
    low = rest - middle
    row = lax.broadcasted_iota(jnp.int32, gain.shape, 0)
    coded = jnp.where(row == 0, high, jnp.where(row == 1, middle, low)).astype(BF)
    mid[...] = x
    for i in range(payload.shape[0]):
        payload[i, :rows, :] = x
        payload[i, rows:, :] = coded


def up_second_kernel(x, *refs):
    out = refs[-1]
    n = (len(refs) - 1) // 2
    hid = refs[0].shape[1]
    rows = out.shape[0]
    scaled, sq = [], jnp.zeros((rows, 1), F32)
    for i in range(x.shape[0]):
        xf = x[i, :rows, :].astype(F32)
        coded = x[i, rows:, :].astype(F32)
        gain = coded[0:1] + coded[1:2] + coded[2:3]
        sq += jnp.sum(xf * xf, axis=1, keepdims=True)
        scaled.append((xf * gain).astype(BF))
    scaled = jnp.concatenate(scaled, axis=1)
    depth = refs[0].shape[0]
    for side in range(2):
        acc = jnp.zeros((rows, hid), F32)
        for d in range(n):
            acc += jnp.dot(
                scaled[:, d * depth : (d + 1) * depth], refs[side * n + d][...], preferred_element_type=F32
            )
        out[:, side * hid : (side + 1) * hid] = acc.astype(BF)
    out[:, 2 * hid :] = stat_columns(sq)


def finish_second_kernel(parts, kept, out):
    out[...] = (0.5 * kept[...].astype(F32) + summed(parts)).astype(BF)


def assemble_kernel(own, other, out):
    chunks, rows, _ = own.shape
    n = chunks // 2
    y, c = lax.axis_index("y"), lax.axis_index("c")
    for side, ref in ((c, own), (1 - c, other)):
        for d in range(n):
            start = pl.multiple_of((side * n + lax.rem(y + d, n)) * rows, rows)
            out[pl.ds(start, rows), :LANES] = ref[2 * d]
            out[pl.ds(start, rows), LANES:] = ref[2 * d + 1]


def spread(x, peers):
    return jnp.broadcast_to(x[None], (peers, *x.shape))


def after(w, done):
    return lax.optimization_barrier((w, done))


def around(w):
    own = [w] + [along_y(w, d) for d in range(1, lax.axis_size("y"))]
    return own + [from_other_core(v) for v in own]


def body(tokens, gain_first, up_first, down_first, gain_second, up_second, down_second):
    ny, nx, nz = lax.axis_size("y"), lax.axis_size("x"), lax.axis_size("z")
    y, z, c = lax.axis_index("y"), lax.axis_index("z"), lax.axis_index("c")
    count, channels = tokens.shape
    width = channels * ny * nx
    half = count // 2
    per_y = half // ny
    few = per_y // nx
    hid = 2 * up_first.shape[1]
    wide = hid + LANES
    activate = call(functools.partial(activate_kernel, width=width), sds((nx, few, hid)))
    down = call(down_kernel, sds((nz, per_y, LANES)))

    payload = call(functools.partial(up_first_kernel, ny=ny, nx=nx), sds((half, wide)))(
        tokens, gain_first[None, :], up_first, from_other_core(up_first)
    )
    parts = exchange(payload.reshape(nx, per_y, wide), "x")
    downs = around(down_first)
    payload = call(pass_on_kernel, sds((per_y, wide)))(parts)
    hidden = activate(exchange(payload.reshape(ny, few, wide), "y"))

    start = c * half + lax.rem(y + z // 2, ny) * per_y
    column = lax.rem(z, 2) * LANES
    kept = lax.dynamic_slice(tokens, (start, column), (per_y, LANES)).astype(F32)
    gain = lax.dynamic_slice(gain_second, (column,), (LANES,))
    kept = by_plane(jnp.concatenate([kept, spread(gain, 8)], axis=0), 1)

    up_second, hidden = after(up_second, hidden)
    ups = around(up_second)
    branch = down(exchange(hidden, "x").reshape(per_y, hid), *downs)
    down_second, branch = after(down_second, branch)
    downs = around(down_second)
    middle, payload = call(finish_first_kernel, (sds((per_y, LANES)), sds((nz, per_y + 8, LANES))))(
        exchange(branch, "z"), kept
    )
    payload = call(up_second_kernel, sds((per_y, wide)))(exchange(payload, "z"), *ups)
    hidden = activate(exchange(payload.reshape(nx, few, wide), "x"))
    branch = down(exchange(hidden, "x").reshape(per_y, hid), *downs)
    finished = call(finish_second_kernel, sds((per_y, LANES)))(exchange(branch, "z"), middle)
    rows = exchange(spread(by_plane(finished, -1), nz), "z")
    return call(assemble_kernel, sds((count, channels)))(rows, from_other_core(rows))


def solution(mesh):
    fine = Mesh(mesh.devices.reshape(4, 4, 8, 2), ("y", "x", "z", "c"))
    cb = ("z", "c")
    placed = (
        P(None, RA),
        P(RA),
        P(RA, cb),
        P(cb, RA),
        P(RA),
        P(RA, cb),
        P(cb, RA),
    )
    return jax.shard_map(body, mesh=fine, in_specs=placed, out_specs=P(None, RA), check_vma=False)
```

```python
import functools

import jax
import jax.numpy as jnp
from jax import lax
from jax.experimental import pallas as pl
from jax.experimental.pallas import tpu as pltpu
from jax.sharding import Mesh, PartitionSpec as P


RA = ("y", "x")
BF = jnp.bfloat16
F32 = jnp.float32
LANES = 128
EPS = 1e-06


def exchange(parts, axis):
    return lax.all_to_all(parts, axis, 0, 0, tiled=True)


def from_other_core(w):
    return lax.ppermute(w, "c", [(0, 1), (1, 0)])


def along_y(a, shift):
    n = lax.axis_size("y")
    return lax.ppermute(a, "y", [(i, (i + shift) % n) for i in range(n)])


def by_plane(a, sign):
    ny, nz = lax.axis_size("y"), lax.axis_size("z")
    perm = [(y * nz + z, (y + sign * (z // 2)) % ny * nz + z) for y in range(ny) for z in range(nz)]
    return lax.ppermute(a, ("y", "z"), perm)


def call(kernel, out, scratch=(), limit=16, whole=None):
    vmem = pl.BlockSpec(memory_space=pltpu.VMEM)
    lies = pl.BlockSpec(memory_space=pltpu.HBM)

    def run(*args):
        first = len(args) if whole is None else whole
        return pl.pallas_call(
            kernel,
            out_shape=out,
            in_specs=[vmem] * first + [lies] * (len(args) - first),
            out_specs=jax.tree.map(lambda _: vmem, out),
            scratch_shapes=list(scratch),
            compiler_params=pltpu.CompilerParams(vmem_limit_bytes=limit << 20),
        )(*args)

    return run


def sds(shape, dtype=BF):
    return jax.ShapeDtypeStruct(shape, dtype)


def stat_columns(sq):
    high = sq.astype(BF)
    low = (sq - high.astype(F32)).astype(BF)
    lane = lax.broadcasted_iota(jnp.int32, (sq.shape[0], LANES), 1)
    block = jnp.where(lane == 0, high.astype(F32), jnp.where(lane == 1, low.astype(F32), 0.0))
    return block.astype(BF)


def fetch(sources, held, sems):
    copies = [pltpu.make_async_copy(w, held.at[i], sems.at[i]) for i, w in enumerate(sources)]
    for copy in copies:
        copy.start()
    return copies


def up_first_kernel(tokens, gain, own, other, out, x, g, held, sems, few_sems):
    half, hid = x.shape[0], own.shape[1]
    start = pl.multiple_of(lax.axis_index("c") * half, half)
    first = [
        pltpu.make_async_copy(tokens.at[pl.ds(start, half), :], x, few_sems.at[0]),
        pltpu.make_async_copy(gain, g, few_sems.at[1]),
    ]
    for copy in first:
        copy.start()
    copies = fetch((own, other), held, sems)
    for copy in first:
        copy.wait()
    xf = x[...].astype(F32)
    out[:, 2 * hid :] = stat_columns(jnp.sum(xf * xf, axis=1, keepdims=True))
    scaled = (xf * g[...]).astype(BF)
    for i, copy in enumerate(copies):
        copy.wait()
        out[:, i * hid : (i + 1) * hid] = jnp.dot(scaled, held[i], preferred_element_type=F32).astype(BF)


def summed(parts):
    total = parts[0].astype(F32)
    for i in range(1, parts.shape[0]):
        total += parts[i].astype(F32)
    return total


def activate_kernel(parts, out, *, width):
    hid = parts.shape[2] - LANES
    total = summed(parts)
    meansq = (total[:, hid : hid + 1] + total[:, hid + 1 : hid + 2]) / width
    act = jnp.maximum(total[:, :hid] * lax.rsqrt(meansq + EPS), 0.0)
    act = (act * act).astype(BF)
    for i in range(out.shape[0]):
        out[i] = act


def down_kernel(hidden, *refs):
    *blocks, out, held, sems = refs
    copies = fetch(blocks, held, sems)
    n = len(blocks) // 2
    k = blocks[0].shape[0]
    for d in range(n):
        copies[d].wait()
        acc = jnp.dot(hidden[:, :k], held[d], preferred_element_type=F32)
        copies[n + d].wait()
        acc += jnp.dot(hidden[:, k:], held[n + d], preferred_element_type=F32)
        acc = acc.astype(BF)
        out[2 * d] = acc[:, :LANES]
        out[2 * d + 1] = acc[:, LANES:]


def finish_first_kernel(parts, kept, mid, payload):
    rows = mid.shape[0]
    x = (0.5 * kept[:rows, :] + summed(parts)).astype(BF)
    gain = kept[rows:, :]
    high = gain.astype(BF).astype(F32)
    rest = gain - high
    middle = rest.astype(BF).astype(F32)
    low = rest - middle
    row = lax.broadcasted_iota(jnp.int32, gain.shape, 0)
    coded = jnp.where(row == 0, high, jnp.where(row == 1, middle, low)).astype(BF)
    mid[...] = x
    for i in range(payload.shape[0]):
        payload[i, :rows, :] = x
        payload[i, rows:, :] = coded


def up_second_kernel(x, *refs):
    *blocks, out, held, sems = refs
    copies = fetch(blocks, held, sems)
    n = len(blocks) // 2
    depth, hid = blocks[0].shape
    rows = out.shape[0]
    scaled, sq = [], jnp.zeros((rows, 1), F32)
    for i in range(x.shape[0]):
        xf = x[i, :rows, :].astype(F32)
        coded = x[i, rows:, :].astype(F32)
        gain = coded[0:1] + coded[1:2] + coded[2:3]
        sq += jnp.sum(xf * xf, axis=1, keepdims=True)
        scaled.append((xf * gain).astype(BF))
    scaled = jnp.concatenate(scaled, axis=1)
    for side in range(2):
        acc = jnp.zeros((rows, hid), F32)
        for d in range(n):
            copies[side * n + d].wait()
            acc += jnp.dot(
                scaled[:, d * depth : (d + 1) * depth], held[side * n + d], preferred_element_type=F32
            )
        out[:, side * hid : (side + 1) * hid] = acc.astype(BF)
    out[:, 2 * hid :] = stat_columns(sq)


def finish_second_kernel(parts, kept, out):
    out[...] = (0.5 * kept[...].astype(F32) + summed(parts)).astype(BF)


def assemble_kernel(own, other, out):
    chunks, rows, _ = own.shape
    n = chunks // 2
    y, c = lax.axis_index("y"), lax.axis_index("c")
    for side, ref in ((c, own), (1 - c, other)):
        for d in range(n):
            start = pl.multiple_of((side * n + lax.rem(y + d, n)) * rows, rows)
            out[pl.ds(start, rows), :LANES] = ref[2 * d]
            out[pl.ds(start, rows), LANES:] = ref[2 * d + 1]


def spread(x, peers):
    return jnp.broadcast_to(x[None], (peers, *x.shape))


def after(w, done):
    return lax.optimization_barrier((w, done))


def around(w):
    own = [w] + [along_y(w, d) for d in range(1, lax.axis_size("y"))]
    return own + [from_other_core(v) for v in own]


def body(tokens, gain_first, up_first, down_first, gain_second, up_second, down_second):
    ny, nx, nz = lax.axis_size("y"), lax.axis_size("x"), lax.axis_size("z")
    y, z, c = lax.axis_index("y"), lax.axis_index("z"), lax.axis_index("c")
    count, channels = tokens.shape
    width = channels * ny * nx
    half = count // 2
    per_y = half // ny
    few = per_y // nx
    hid = 2 * up_first.shape[1]
    wide = hid + LANES
    blocks = 2 * ny

    def held(n, w):
        return [pltpu.VMEM((n, *w.shape), BF), pltpu.SemaphoreType.DMA((n,))]

    activate = call(functools.partial(activate_kernel, width=width), sds((nx, few, hid)))
    down = call(down_kernel, sds((nz, per_y, LANES)), held(blocks, down_first), whole=1)

    arrays = [pltpu.VMEM((half, channels), BF), pltpu.VMEM((1, channels), F32)]
    scratch = arrays + held(2, up_first) + [pltpu.SemaphoreType.DMA((2,))]
    payload = call(up_first_kernel, sds((half, wide)), scratch, whole=0)(
        tokens, gain_first[None, :], up_first, from_other_core(up_first)
    )
    start = c * half + lax.rem(y + z // 2, ny) * per_y
    column = lax.rem(z, 2) * LANES
    kept = lax.dynamic_slice(tokens, (start, column), (per_y, LANES)).astype(F32)
    gain = lax.dynamic_slice(gain_second, (column,), (LANES,))
    kept = jnp.concatenate([kept, spread(gain, 8)], axis=0)
    kept, payload = after(kept, payload)
    parts = exchange(payload.reshape(ny * nx, few, wide), RA)
    kept = by_plane(kept, 1)
    down_first, kept = after(down_first, kept)
    downs = around(down_first)
    hidden = activate(parts)

    hidden = exchange(hidden, "x").reshape(per_y, hid)
    ups = around(up_second)
    branch = down(hidden, *downs)
    branch = exchange(branch, "z")
    downs = around(down_second)
    middle, payload = call(finish_first_kernel, (sds((per_y, LANES)), sds((nz, per_y + 8, LANES))))(
        branch, kept
    )
    payload = exchange(payload, "z")
    payload = call(up_second_kernel, sds((per_y, wide)), held(blocks, up_second), whole=1)(payload, *ups)
    parts = exchange(payload.reshape(nx, few, wide), "x")
    hidden = activate(parts)
    hidden = exchange(hidden, "x").reshape(per_y, hid)
    branch = down(hidden, *downs)
    finished = call(finish_second_kernel, sds((per_y, LANES)))(exchange(branch, "z"), middle)
    rows = exchange(spread(by_plane(finished, -1), nz), "z")
    return call(assemble_kernel, sds((count, channels)))(rows, from_other_core(rows))


def solution(mesh):
    fine = Mesh(mesh.devices.reshape(4, 4, 8, 2), ("y", "x", "z", "c"))
    cb = ("z", "c")
    placed = (
        P(None, RA),
        P(RA),
        P(RA, cb),
        P(cb, RA),
        P(RA),
        P(RA, cb),
        P(cb, RA),
    )

    return jax.shard_map(body, mesh=fine, in_specs=placed, out_specs=P(None, RA), check_vma=False)
```

```python
import functools

import jax
import jax.numpy as jnp
from jax import lax
from jax.experimental import pallas as pl
from jax.experimental.pallas import tpu as pltpu
from jax.sharding import Mesh, PartitionSpec as P


RA = ("y", "x")
BF = jnp.bfloat16
F32 = jnp.float32
LANES = 128
EPS = 1e-06


def exchange(parts, axis):
    return lax.all_to_all(parts, axis, 0, 0, tiled=True)


def from_other_core(w):
    return lax.ppermute(w, "c", [(0, 1), (1, 0)])


def along_y(a, shift):
    n = lax.axis_size("y")
    return lax.ppermute(a, "y", [(i, (i + shift) % n) for i in range(n)])


def by_plane(a, steps):
    ny, nz = lax.axis_size("y"), lax.axis_size("z")
    perm = [(y * nz + z, (y + steps(z)) % ny * nz + z) for y in range(ny) for z in range(nz)]
    return lax.ppermute(a, ("y", "z"), perm)


def call(kernel, out, scratch=(), limit=16, whole=None, update=None):
    vmem = pl.BlockSpec(memory_space=pltpu.VMEM)
    lies = pl.BlockSpec(memory_space=pltpu.HBM if update is None else pl.ANY)

    def run(*args):
        first = len(args) if whole is None else whole
        if update is None:
            args = [*args[:first], *(pltpu.with_memory_space_constraint(a, pltpu.HBM) for a in args[first:])]
        return pl.pallas_call(
            kernel,
            out_shape=out,
            in_specs=[vmem] * first + [lies] * (len(args) - first),
            out_specs=jax.tree.map(lambda _: vmem if update is None else lies, out),
            scratch_shapes=list(scratch),
            input_output_aliases={} if update is None else {update: 0},
            compiler_params=pltpu.CompilerParams(vmem_limit_bytes=limit << 20),
        )(*args)

    return run


def sds(shape, dtype=BF):
    return jax.ShapeDtypeStruct(shape, dtype)


def stat_columns(sq):
    high = sq.astype(BF)
    low = (sq - high.astype(F32)).astype(BF)
    lane = lax.broadcasted_iota(jnp.int32, (sq.shape[0], LANES), 1)
    block = jnp.where(lane == 0, high.astype(F32), jnp.where(lane == 1, low.astype(F32), 0.0))
    return block.astype(BF)


def fetch(pairs, sems):
    copies = [pltpu.make_async_copy(source, held, sems.at[i]) for i, (source, held) in enumerate(pairs)]
    for copy in copies:
        copy.start()
    return copies


def up_own_kernel(gain, next_gain, tokens, own, out, scaled, kept, x, some, w, sems):
    half, hid = x.shape[0], own.shape[1]
    rows = some.shape[0]
    y, z, c = lax.axis_index("y"), lax.axis_index("z"), lax.axis_index("c")
    first = pl.multiple_of(c * half, half)
    there = lax.rem(y + z // 2, lax.axis_size("y"))
    copies = fetch(
        (
            (tokens.at[pl.ds(first, half), :], x),
            (own, w),
            (tokens.at[pl.ds(pl.multiple_of(first + there * rows, rows), rows), :], some),
        ),
        sems,
    )
    copies[0].wait()
    xf = x[...].astype(F32)
    out[:, 2 * hid :] = stat_columns(jnp.sum(xf * xf, axis=1, keepdims=True))
    scaled[...] = (xf * gain[...]).astype(BF)
    copies[1].wait()
    out[:, :hid] = jnp.dot(scaled[...], w[...], preferred_element_type=F32).astype(BF)
    copies[2].wait()
    left = lax.rem(z, 2) == 0
    kept[:rows, :] = jnp.where(left, some[:, :LANES].astype(F32), some[:, LANES:].astype(F32))
    chosen = jnp.where(left, next_gain[:, :LANES], next_gain[:, LANES:])
    kept[rows:, :] = jnp.broadcast_to(chosen, (8, LANES))


def up_other_kernel(scaled, other, so_far, out, w, part, sems):
    del so_far
    hid = other.shape[1]
    fetch(((other, w),), sems)[0].wait()
    part[...] = jnp.dot(scaled[...], w[...], preferred_element_type=F32).astype(BF)
    fetch(((part, out.at[:, hid : 2 * hid]),), sems)[0].wait()


def summed(parts):
    total = parts[0].astype(F32)
    for i in range(1, parts.shape[0]):
        total += parts[i].astype(F32)
    return total


def activate_kernel(parts, out, *, width):
    hid = parts.shape[2] - LANES
    total = summed(parts)
    meansq = (total[:, hid : hid + 1] + total[:, hid + 1 : hid + 2]) / width
    act = jnp.maximum(total[:, :hid] * lax.rsqrt(meansq + EPS), 0.0)
    act = (act * act).astype(BF)
    for i in range(out.shape[0]):
        out[i] = act


def spots(blocks, held):
    pairs, i = [], 0
    for block in blocks:
        if isinstance(block, tuple):
            rows = block[0].shape[0]
            pairs += [(block[0], held.at[i, :rows]), (block[1], held.at[i, rows:])]
        else:
            pairs.append((block, held.at[i]))
        i += 1
    return pairs


def grouped(refs, n):
    if len(refs) == n:
        return list(refs)
    middle = n // 2
    return [*refs[:middle], (refs[middle], refs[middle + 1]), *refs[middle + 2 :]]


def down_kernel(hidden, *refs):
    *blocks, out, held, sems = refs
    n, k = held.shape[0] // 2, held.shape[1]
    per = len(blocks) // 2
    copies = fetch(spots(grouped(blocks[:per], n) + grouped(blocks[per:], n), held), sems)
    waited = [0, 0]

    def ready(side, d):
        upto = per if d == n - 1 else (d + 1 if d < n // 2 else d + 1 + per - n)
        for i in range(waited[side], upto):
            copies[side * per + i].wait()
        waited[side] = upto
        return held[side * n + d]

    for d in range(n):
        acc = jnp.dot(hidden[:, :k], ready(0, d), preferred_element_type=F32)
        acc += jnp.dot(hidden[:, k:], ready(1, d), preferred_element_type=F32)
        acc = acc.astype(BF)
        out[2 * d] = acc[:, :LANES]
        out[2 * d + 1] = acc[:, LANES:]


def finish_first_kernel(parts, kept, mid, payload):
    rows = mid.shape[0]
    x = (0.5 * kept[:rows, :] + summed(parts)).astype(BF)
    gain = kept[rows:, :]
    high = gain.astype(BF).astype(F32)
    rest = gain - high
    middle = rest.astype(BF).astype(F32)
    low = rest - middle
    row = lax.broadcasted_iota(jnp.int32, gain.shape, 0)
    coded = jnp.where(row == 0, high, jnp.where(row == 1, middle, low)).astype(BF)
    mid[...] = x
    for i in range(payload.shape[0]):
        payload[i, :rows, :] = x
        payload[i, rows:, :] = coded


def up_second_kernel(x, *refs):
    *blocks, out, held, sems = refs
    copies = fetch(spots(blocks, held), sems)
    n = len(blocks) // 2
    depth, hid = blocks[0].shape
    rows = out.shape[0]
    scaled, sq = [], jnp.zeros((rows, 1), F32)
    for i in range(x.shape[0]):
        xf = x[i, :rows, :].astype(F32)
        coded = x[i, rows:, :].astype(F32)
        gain = coded[0:1] + coded[1:2] + coded[2:3]
        sq += jnp.sum(xf * xf, axis=1, keepdims=True)
        scaled.append((xf * gain).astype(BF))
    scaled = jnp.concatenate(scaled, axis=1)
    for side in range(2):
        acc = jnp.zeros((rows, hid), F32)
        for d in range(n):
            copies[side * n + d].wait()
            acc += jnp.dot(
                scaled[:, d * depth : (d + 1) * depth], held[side * n + d], preferred_element_type=F32
            )
        out[:, side * hid : (side + 1) * hid] = acc.astype(BF)
    out[:, 2 * hid :] = stat_columns(sq)


def finish_second_kernel(parts, kept, out):
    out[...] = (0.5 * kept[...].astype(F32) + summed(parts)).astype(BF)


def assemble_kernel(own, other, out):
    chunks, rows, _ = own.shape
    n = chunks // 2
    y, c = lax.axis_index("y"), lax.axis_index("c")
    for side, ref in ((c, own), (1 - c, other)):
        for d in range(n):
            start = pl.multiple_of((side * n + lax.rem(y + d, n)) * rows, rows)
            out[pl.ds(start, rows), :LANES] = ref[2 * d]
            out[pl.ds(start, rows), LANES:] = ref[2 * d + 1]


def spread(x, peers):
    return jnp.broadcast_to(x[None], (peers, *x.shape))


def after(w, done):
    return lax.optimization_barrier((w, done))


def around(w, forward=False):
    n = lax.axis_size("y")
    own = [w] + [along_y(w, d) for d in range(1, n) if not (forward and d == n // 2)]
    if forward:
        half = w.shape[0] // 2
        far = [along_y(own[1][:half], 1), along_y(own[-1][half:], n - 1)]
        own[n // 2 : n // 2] = far
    return own + [from_other_core(v) for v in own]


def body(tokens, gain_first, up_first, down_first, gain_second, up_second, down_second):
    ny, nx, nz = lax.axis_size("y"), lax.axis_size("x"), lax.axis_size("z")
    count, channels = tokens.shape
    width = channels * ny * nx
    half = count // 2
    per_y = half // ny
    few = per_y // nx
    hid = 2 * up_first.shape[1]
    wide = hid + LANES
    blocks = 2 * ny

    def held(w, more=0):
        return [pltpu.VMEM((blocks, *w.shape), BF), pltpu.SemaphoreType.DMA((blocks + more,))]

    activate = call(functools.partial(activate_kernel, width=width), sds((nx, few, hid)))

    block = pltpu.VMEM(up_first.shape, BF)
    payload, scaled, kept = call(
        up_own_kernel,
        (sds((half, wide)), sds((half, channels)), sds((per_y + 8, LANES), F32)),
        [pltpu.VMEM((half, channels), BF), pltpu.VMEM((per_y, channels), BF), block, pltpu.SemaphoreType.DMA((3,))],
        whole=2,
    )(gain_first[None, :], gain_second[None, :], tokens, up_first)
    payload = call(
        up_other_kernel,
        sds((half, wide)),
        [block, pltpu.VMEM((half, hid // 2), BF), pltpu.SemaphoreType.DMA((1,))],
        whole=1,
        update=2,
    )(scaled, from_other_core(up_first), payload)
    parts = exchange(payload.reshape(ny * nx, few, wide), RA)
    kept = by_plane(kept, lambda z: max(z // 2, 1))
    kept = by_plane(kept, lambda z: -1 if z < 2 else 0)
    down_first, kept = after(down_first, kept)
    downs = around(down_first, forward=True)
    hidden = activate(parts)

    hidden = exchange(hidden, "x").reshape(per_y, hid)
    ups = around(up_second)
    branch = call(down_kernel, sds((nz, per_y, LANES)), held(down_first, 2), whole=1)(hidden, *downs)
    branch = exchange(branch, "z")
    downs = around(down_second)
    middle, payload = call(finish_first_kernel, (sds((per_y, LANES)), sds((nz, per_y + 8, LANES))))(
        branch, kept
    )
    payload = exchange(payload, "z")
    payload = call(up_second_kernel, sds((per_y, wide)), held(up_second), whole=1)(payload, *ups)
    parts = exchange(payload.reshape(nx, few, wide), "x")
    hidden = activate(parts)
    hidden = exchange(hidden, "x").reshape(per_y, hid)
    branch = call(down_kernel, sds((nz, per_y, LANES)), held(down_second), whole=1)(hidden, *downs)
    finished = call(finish_second_kernel, sds((per_y, LANES)))(exchange(branch, "z"), middle)
    rows = exchange(spread(by_plane(finished, lambda z: -(z // 2)), nz), "z")
    return call(assemble_kernel, sds((count, channels)))(rows, from_other_core(rows))


def solution(mesh):
    fine = Mesh(mesh.devices.reshape(4, 4, 8, 2), ("y", "x", "z", "c"))
    cb = ("z", "c")
    placed = (
        P(None, RA),
        P(RA),
        P(RA, cb),
        P(cb, RA),
        P(RA),
        P(RA, cb),
        P(cb, RA),
    )

    return jax.shard_map(body, mesh=fine, in_specs=placed, out_specs=P(None, RA), check_vma=False)
```

```python
import functools

import jax
import jax.numpy as jnp
from jax import lax
from jax.experimental import pallas as pl
from jax.experimental.pallas import tpu as pltpu
from jax.sharding import Mesh, PartitionSpec as P


RA = ("y", "x")
BF = jnp.bfloat16
F32 = jnp.float32
LANES = 128
EPS = 1e-06


def exchange(parts, axis):
    return lax.all_to_all(parts, axis, 0, 0, tiled=True)


def from_other_core(w):
    return lax.ppermute(w, "c", [(0, 1), (1, 0)])


def along_y(a, shift):
    n = lax.axis_size("y")
    return lax.ppermute(a, "y", [(i, (i + shift) % n) for i in range(n)])


def by_plane(a, steps):
    ny, nz = lax.axis_size("y"), lax.axis_size("z")
    perm = [(y * nz + z, (y + steps(z)) % ny * nz + z) for y in range(ny) for z in range(nz)]
    return lax.ppermute(a, ("y", "z"), perm)


def call(kernel, out, scratch=(), limit=16, whole=None, update=None):
    vmem = pl.BlockSpec(memory_space=pltpu.VMEM)
    lies = pl.BlockSpec(memory_space=pltpu.HBM if update is None else pl.ANY)

    def run(*args):
        first = len(args) if whole is None else whole
        if update is None:
            args = [*args[:first], *(pltpu.with_memory_space_constraint(a, pltpu.HBM) for a in args[first:])]
        return pl.pallas_call(
            kernel,
            out_shape=out,
            in_specs=[vmem] * first + [lies] * (len(args) - first),
            out_specs=jax.tree.map(lambda _: vmem if update is None else lies, out),
            scratch_shapes=list(scratch),
            input_output_aliases={} if update is None else {update: 0},
            compiler_params=pltpu.CompilerParams(vmem_limit_bytes=limit << 20),
        )(*args)

    return run


def sds(shape, dtype=BF):
    return jax.ShapeDtypeStruct(shape, dtype)


def stat_columns(sq):
    high = sq.astype(BF)
    low = (sq - high.astype(F32)).astype(BF)
    lane = lax.broadcasted_iota(jnp.int32, (sq.shape[0], LANES), 1)
    block = jnp.where(lane == 0, high.astype(F32), jnp.where(lane == 1, low.astype(F32), 0.0))
    return block.astype(BF)


def fetch(pairs, sems):
    copies = [pltpu.make_async_copy(source, held, sems.at[i]) for i, (source, held) in enumerate(pairs)]
    for copy in copies:
        copy.start()
    return copies


def up_own_kernel(gain, next_gain, tokens, own, out, scaled, kept, x, some, w, sems):
    half, hid = x.shape[0], own.shape[1]
    rows = some.shape[0]
    y, z, c = lax.axis_index("y"), lax.axis_index("z"), lax.axis_index("c")
    first = pl.multiple_of(c * half, half)
    there = lax.rem(y + z // 2, lax.axis_size("y"))
    copies = fetch(
        (
            (tokens.at[pl.ds(first, half), :], x),
            (own, w),
            (tokens.at[pl.ds(pl.multiple_of(first + there * rows, rows), rows), :], some),
        ),
        sems,
    )
    copies[0].wait()
    xf = x[...].astype(F32)
    out[:, 2 * hid :] = stat_columns(jnp.sum(xf * xf, axis=1, keepdims=True))
    scaled[...] = (xf * gain[...]).astype(BF)
    copies[1].wait()
    out[:, :hid] = jnp.dot(scaled[...], w[...], preferred_element_type=F32).astype(BF)
    copies[2].wait()
    left = lax.rem(z, 2) == 0
    kept[:rows, :] = jnp.where(left, some[:, :LANES].astype(F32), some[:, LANES:].astype(F32))
    chosen = jnp.where(left, next_gain[:, :LANES], next_gain[:, LANES:])
    kept[rows:, :] = jnp.broadcast_to(chosen, (8, LANES))


def up_other_kernel(scaled, other, so_far, out, w, part, sems):
    del so_far
    hid = other.shape[1]
    fetch(((other, w),), sems)[0].wait()
    part[...] = jnp.dot(scaled[...], w[...], preferred_element_type=F32).astype(BF)
    fetch(((part, out.at[:, hid : 2 * hid]),), sems)[0].wait()


def summed(parts):
    total = parts[0].astype(F32)
    for i in range(1, parts.shape[0]):
        total += parts[i].astype(F32)
    return total


def activate_kernel(parts, out, *, width):
    hid = parts.shape[2] - LANES
    total = summed(parts)
    meansq = (total[:, hid : hid + 1] + total[:, hid + 1 : hid + 2]) / width
    act = jnp.maximum(total[:, :hid] * lax.rsqrt(meansq + EPS), 0.0)
    act = (act * act).astype(BF)
    for i in range(out.shape[0]):
        out[i] = act


def spots(blocks, held):
    pairs, i = [], 0
    for block in blocks:
        if isinstance(block, tuple):
            rows = block[0].shape[0]
            pairs += [(block[0], held.at[i, :rows]), (block[1], held.at[i, rows:])]
        else:
            pairs.append((block, held.at[i]))
        i += 1
    return pairs


def grouped(refs, n):
    if len(refs) == n:
        return list(refs)
    middle = n // 2
    return [*refs[:middle], (refs[middle], refs[middle + 1]), *refs[middle + 2 :]]


def down_kernel(hidden, *refs):
    *blocks, out, held, sems = refs
    n, k = held.shape[0] // 2, held.shape[1]
    per = len(blocks) // 2
    copies = fetch(spots(grouped(blocks[:per], n) + grouped(blocks[per:], n), held), sems)
    waited = [0, 0]

    def ready(side, d):
        upto = per if d == n - 1 else (d + 1 if d < n // 2 else d + 1 + per - n)
        for i in range(waited[side], upto):
            copies[side * per + i].wait()
        waited[side] = upto
        return held[side * n + d]

    for d in range(n):
        acc = jnp.dot(hidden[:, :k], ready(0, d), preferred_element_type=F32)
        acc += jnp.dot(hidden[:, k:], ready(1, d), preferred_element_type=F32)
        acc = acc.astype(BF)
        out[2 * d] = acc[:, :LANES]
        out[2 * d + 1] = acc[:, LANES:]


def finish_first_kernel(parts, kept, mid, payload):
    rows = mid.shape[0]
    x = (0.5 * kept[:rows, :] + summed(parts)).astype(BF)
    gain = kept[rows:, :]
    high = gain.astype(BF).astype(F32)
    rest = gain - high
    middle = rest.astype(BF).astype(F32)
    low = rest - middle
    row = lax.broadcasted_iota(jnp.int32, gain.shape, 0)
    coded = jnp.where(row == 0, high, jnp.where(row == 1, middle, low)).astype(BF)
    mid[...] = x
    for i in range(payload.shape[0]):
        payload[i, :rows, :] = x
        payload[i, rows:, :] = coded


def up_second_kernel(x, *refs):
    *blocks, out, held, sems = refs
    copies = fetch(spots(blocks, held), sems)
    n = len(blocks) // 2
    depth, hid = blocks[0].shape
    rows = out.shape[0]
    scaled, sq = [], jnp.zeros((rows, 1), F32)
    for i in range(x.shape[0]):
        xf = x[i, :rows, :].astype(F32)
        coded = x[i, rows:, :].astype(F32)
        gain = coded[0:1] + coded[1:2] + coded[2:3]
        sq += jnp.sum(xf * xf, axis=1, keepdims=True)
        scaled.append((xf * gain).astype(BF))
    scaled = jnp.concatenate(scaled, axis=1)
    for side in range(2):
        acc = jnp.zeros((rows, hid), F32)
        for d in range(n):
            copies[side * n + d].wait()
            acc += jnp.dot(
                scaled[:, d * depth : (d + 1) * depth], held[side * n + d], preferred_element_type=F32
            )
        out[:, side * hid : (side + 1) * hid] = acc.astype(BF)
    out[:, 2 * hid :] = stat_columns(sq)


def finish_second_kernel(parts, kept, out):
    out[...] = (0.5 * kept[...].astype(F32) + summed(parts)).astype(BF)


def assemble_kernel(own, other, out):
    chunks, rows, _ = own.shape
    n = chunks // 2
    y, c = lax.axis_index("y"), lax.axis_index("c")
    for side, ref in ((c, own), (1 - c, other)):
        for d in range(n):
            start = pl.multiple_of((side * n + lax.rem(y + d, n)) * rows, rows)
            out[pl.ds(start, rows), :LANES] = ref[2 * d]
            out[pl.ds(start, rows), LANES:] = ref[2 * d + 1]


def spread(x, peers):
    return jnp.broadcast_to(x[None], (peers, *x.shape))


def after(w, done):
    return lax.optimization_barrier((w, done))


def around(w, swapped, forward=False):
    n = lax.axis_size("y")
    own = [w] + [along_y(w, d) for d in range(1, n) if not (forward and d == n // 2)]
    if forward:
        half = w.shape[0] // 2
        far = [along_y(own[1][:half], 1), along_y(own[-1][half:], n - 1)]
        own[n // 2 : n // 2] = far
    return own + [swapped] + [from_other_core(v) for v in own[1:]]


def body(tokens, gain_first, up_first, down_first, gain_second, up_second, down_second):
    ny, nx, nz = lax.axis_size("y"), lax.axis_size("x"), lax.axis_size("z")
    count, channels = tokens.shape
    width = channels * ny * nx
    half = count // 2
    per_y = half // ny
    few = per_y // nx
    hid = 2 * up_first.shape[1]
    wide = hid + LANES
    blocks = 2 * ny

    def held(w, more=0):
        return [pltpu.VMEM((blocks, *w.shape), BF), pltpu.SemaphoreType.DMA((blocks + more,))]

    activate = call(functools.partial(activate_kernel, width=width), sds((nx, few, hid)))

    block = pltpu.VMEM(up_first.shape, BF)
    payload, scaled, kept = call(
        up_own_kernel,
        (sds((half, wide)), sds((half, channels)), sds((per_y + 8, LANES), F32)),
        [pltpu.VMEM((half, channels), BF), pltpu.VMEM((per_y, channels), BF), block, pltpu.SemaphoreType.DMA((3,))],
        whole=2,
    )(gain_first[None, :], gain_second[None, :], tokens, up_first)
    payload = call(
        up_other_kernel,
        sds((half, wide)),
        [block, pltpu.VMEM((half, hid // 2), BF), pltpu.SemaphoreType.DMA((1,))],
        whole=1,
        update=2,
    )(scaled, from_other_core(up_first), payload)
    parts = exchange(payload.reshape(ny * nx, few, wide), RA)
    kept = by_plane(kept, lambda z: z // 2)
    swapped, order = [], payload
    for w in (down_second, up_second, down_first):
        w, order = after(w, order)
        order = from_other_core(w)
        swapped.append(order)
    down_first, order = after(down_first, order)
    downs = around(down_first, order, forward=True)
    hidden = activate(parts)

    hidden = exchange(hidden, "x").reshape(per_y, hid)
    ups = around(up_second, swapped[1])
    branch = call(down_kernel, sds((nz, per_y, LANES)), held(down_first, 2), whole=1)(hidden, *downs)
    branch = exchange(branch, "z")
    downs = around(down_second, swapped[0])
    middle, payload = call(finish_first_kernel, (sds((per_y, LANES)), sds((nz, per_y + 8, LANES))))(
        branch, kept
    )
    payload = exchange(payload, "z")
    payload = call(up_second_kernel, sds((per_y, wide)), held(up_second), whole=1)(payload, *ups)
    parts = exchange(payload.reshape(nx, few, wide), "x")
    hidden = activate(parts)
    hidden = exchange(hidden, "x").reshape(per_y, hid)
    branch = call(down_kernel, sds((nz, per_y, LANES)), held(down_second), whole=1)(hidden, *downs)
    finished = call(finish_second_kernel, sds((per_y, LANES)))(exchange(branch, "z"), middle)
    rows = exchange(spread(by_plane(finished, lambda z: -(z // 2)), nz), "z")
    return call(assemble_kernel, sds((count, channels)))(rows, from_other_core(rows))


def solution(mesh):
    fine = Mesh(mesh.devices.reshape(4, 4, 8, 2), ("y", "x", "z", "c"))
    cb = ("z", "c")
    placed = (
        P(None, RA),
        P(RA),
        P(RA, cb),
        P(cb, RA),
        P(RA),
        P(RA, cb),
        P(cb, RA),
    )

    return jax.shard_map(body, mesh=fine, in_specs=placed, out_specs=P(None, RA), check_vma=False)
```

```python
import functools

import jax
import jax.numpy as jnp
from jax import lax
from jax.experimental import pallas as pl
from jax.experimental.pallas import tpu as pltpu
from jax.sharding import Mesh, PartitionSpec as P


RA = ("y", "x")
BF = jnp.bfloat16
F32 = jnp.float32
LANES = 128
EPS = 1e-06


def exchange(parts, axis):
    return lax.all_to_all(parts, axis, 0, 0, tiled=True)


def from_other_core(w):
    return lax.ppermute(w, "c", [(0, 1), (1, 0)])


def along_y(a, shift):
    n = lax.axis_size("y")
    return lax.ppermute(a, "y", [(i, (i + shift) % n) for i in range(n)])


def along_x(a, shift):
    n = lax.axis_size("x")
    return lax.ppermute(a, "x", [(i, (i + shift) % n) for i in range(n)])


def by_plane(a, steps):
    ny, nz = lax.axis_size("y"), lax.axis_size("z")
    perm = [(y * nz + z, (y + steps(z)) % ny * nz + z) for y in range(ny) for z in range(nz)]
    return lax.ppermute(a, ("y", "z"), perm)


def call(kernel, out, scratch=(), limit=16, whole=None, update=None):
    vmem = pl.BlockSpec(memory_space=pltpu.VMEM)
    lies = pl.BlockSpec(memory_space=pltpu.HBM if update is None else pl.ANY)

    def run(*args):
        first = len(args) if whole is None else whole
        if update is None:
            args = [*args[:first], *(pltpu.with_memory_space_constraint(a, pltpu.HBM) for a in args[first:])]
        return pl.pallas_call(
            kernel,
            out_shape=out,
            in_specs=[vmem] * first + [lies] * (len(args) - first),
            out_specs=jax.tree.map(lambda _: vmem if update is None else lies, out),
            scratch_shapes=list(scratch),
            input_output_aliases={} if update is None else {update: 0},
            compiler_params=pltpu.CompilerParams(vmem_limit_bytes=limit << 20),
        )(*args)

    return run


def sds(shape, dtype=BF):
    return jax.ShapeDtypeStruct(shape, dtype)


def stat_columns(sq):
    high = sq.astype(BF)
    low = (sq - high.astype(F32)).astype(BF)
    lane = lax.broadcasted_iota(jnp.int32, (sq.shape[0], LANES), 1)
    block = jnp.where(lane == 0, high.astype(F32), jnp.where(lane == 1, low.astype(F32), 0.0))
    return block.astype(BF)


def fetch(pairs, sems):
    copies = [pltpu.make_async_copy(source, held, sems.at[i]) for i, (source, held) in enumerate(pairs)]
    for copy in copies:
        copy.start()
    return copies


def up_own_kernel(tokens, gain, next_gain, own, out, scaled, kept, x, g, g2, some, some_f, w, sems):
    half, hid = x.shape[0], own.shape[1]
    rows = some.shape[0]
    nx, few, _ = some_f.shape
    y, z, c = lax.axis_index("y"), lax.axis_index("z"), lax.axis_index("c")
    first = pl.multiple_of(c * half, half)
    there = lax.rem(y + z // 2, lax.axis_size("y"))
    copies = fetch(
        (
            (gain, g),
            (tokens.at[pl.ds(first, half), :], x),
            (own, w),
            (tokens.at[pl.ds(pl.multiple_of(first + there * rows, rows), rows), :], some),
            (next_gain, g2),
        ),
        sems,
    )
    copies[0].wait()
    copies[1].wait()
    xf = x[...].astype(F32)
    out[:, 2 * hid :] = stat_columns(jnp.sum(xf * xf, axis=1, keepdims=True))
    scaled[...] = (xf * g[...]).astype(BF)
    copies[2].wait()
    out[:, :hid] = jnp.dot(scaled[...], w[...], preferred_element_type=F32).astype(BF)
    copies[3].wait()
    copies[4].wait()
    left = lax.rem(z, 2) == 0
    chosen = jnp.where(left, some[:, :LANES].astype(F32), some[:, LANES:].astype(F32))
    for i in range(nx):
        some_f[i] = chosen[i * few : (i + 1) * few]
    for j in range(nx):
        kept[j * few : (j + 1) * few, :] = some_f[lax.rem(lax.axis_index("x") + nx - j, nx)]
    chosen = jnp.where(left, g2[:, :LANES], g2[:, LANES:])
    kept[rows:, :] = jnp.broadcast_to(chosen, (8, LANES))


def up_other_kernel(scaled, other, so_far, out, w, part, sems):
    del so_far
    hid = other.shape[1]
    fetch(((other, w),), sems)[0].wait()
    part[...] = jnp.dot(scaled[...], w[...], preferred_element_type=F32).astype(BF)
    fetch(((part, out.at[:, hid : 2 * hid]),), sems)[0].wait()


def summed(parts):
    total = parts[0][...].astype(F32)
    for i in range(1, len(parts) if isinstance(parts, list) else parts.shape[0]):
        total += parts[i][...].astype(F32)
    return total


def activate_kernel(*refs, width):
    *parts, out = refs
    hid = out.shape[1]
    total = summed(parts[0] if len(parts) == 1 else parts)
    meansq = (total[:, hid : hid + 1] + total[:, hid + 1 : hid + 2]) / width
    act = jnp.maximum(total[:, :hid] * lax.rsqrt(meansq + EPS), 0.0)
    out[...] = (act * act).astype(BF)


def spots(blocks, held):
    pairs, i = [], 0
    for block in blocks:
        if isinstance(block, tuple):
            rows = block[0].shape[0]
            pairs += [(block[0], held.at[i, :rows]), (block[1], held.at[i, rows:])]
        else:
            pairs.append((block, held.at[i]))
        i += 1
    return pairs


def grouped(refs, n):
    if len(refs) == n:
        return list(refs)
    middle = n // 2
    return [*refs[:middle], (refs[middle], refs[middle + 1]), *refs[middle + 2 :]]


def down_kernel(hidden, *refs):
    *blocks, out, held, sems = refs
    n, k = held.shape[0] // 2, held.shape[1]
    per = len(blocks) // 2
    copies = fetch(spots(grouped(blocks[:per], n) + grouped(blocks[per:], n), held), sems)
    waited = [0, 0]

    def ready(side, d):
        upto = per if d == n - 1 else (d + 1 if d < n // 2 else d + 1 + per - n)
        for i in range(waited[side], upto):
            copies[side * per + i].wait()
        waited[side] = upto
        return held[side * n + d]

    for d in range(n):
        acc = jnp.dot(hidden[:, :k], ready(0, d), preferred_element_type=F32)
        acc += jnp.dot(hidden[:, k:], ready(1, d), preferred_element_type=F32)
        acc = acc.astype(BF)
        out[2 * d] = acc[:, :LANES]
        out[2 * d + 1] = acc[:, LANES:]


def finish_first_kernel(parts, kept, mid, payload):
    rows = mid.shape[0]
    x = (0.5 * kept[:rows, :] + summed(parts)).astype(BF)
    gain = kept[rows:, :]
    high = gain.astype(BF).astype(F32)
    rest = gain - high
    middle = rest.astype(BF).astype(F32)
    low = rest - middle
    row = lax.broadcasted_iota(jnp.int32, gain.shape, 0)
    coded = jnp.where(row == 0, high, jnp.where(row == 1, middle, low)).astype(BF)
    mid[...] = x
    for i in range(payload.shape[0]):
        payload[i, :rows, :] = x
        payload[i, rows:, :] = coded


def up_second_kernel(x, *refs):
    *refs, held, sems = refs
    blocks, outs = refs[: held.shape[0]], refs[held.shape[0] :]
    copies = fetch(spots(blocks, held), sems)
    n = len(blocks) // 2
    depth, hid = blocks[0].shape
    few = outs[0].shape[0]
    rows = few * len(outs)
    scaled, sq = [], jnp.zeros((rows, 1), F32)
    for i in range(x.shape[0]):
        xf = x[i, :rows, :].astype(F32)
        coded = x[i, rows:, :].astype(F32)
        gain = coded[0:1] + coded[1:2] + coded[2:3]
        sq += jnp.sum(xf * xf, axis=1, keepdims=True)
        scaled.append((xf * gain).astype(BF))
    scaled = jnp.concatenate(scaled, axis=1)
    for side in range(2):
        acc = jnp.zeros((rows, hid), F32)
        for d in range(n):
            copies[side * n + d].wait()
            acc += jnp.dot(
                scaled[:, d * depth : (d + 1) * depth], held[side * n + d], preferred_element_type=F32
            )
        for j, out in enumerate(outs):
            out[:, side * hid : (side + 1) * hid] = acc[j * few : (j + 1) * few].astype(BF)
    for j, out in enumerate(outs):
        out[:, 2 * hid :] = stat_columns(sq[j * few : (j + 1) * few])


def finish_second_kernel(parts, kept, out):
    out[...] = (0.5 * kept[...].astype(F32) + summed(parts)).astype(BF)


def assemble_kernel(own, other, out, placed):
    chunks = own.shape[0]
    ny = chunks // 2
    few = placed.shape[1]
    nx = own.shape[1] // few
    x, y, c = lax.axis_index("x"), lax.axis_index("y"), lax.axis_index("c")
    for side, ref in ((c, own), (1 - c, other)):
        for i in range(chunks):
            block = ref[i].astype(F32)
            row = (side * ny + lax.rem(y + i // 2, ny)) * nx
            column = (i % 2) * LANES
            for j in range(nx):
                placed[row + lax.rem(x + nx - j, nx), :, column : column + LANES] = block[j * few : (j + 1) * few]
    out[...] = placed[...].reshape(out.shape).astype(BF)


def spread(x, peers):
    return jnp.broadcast_to(x[None], (peers, *x.shape))


def after(w, done):
    return lax.optimization_barrier((w, done))


def around(w, swapped, forward=False):
    n = lax.axis_size("y")
    own = [w] + [along_y(w, d) for d in range(1, n) if not (forward and d == n // 2)]
    if forward:
        half = w.shape[0] // 2
        far = [along_y(own[1][:half], 1), along_y(own[-1][half:], n - 1)]
        own[n // 2 : n // 2] = far
    return own + [swapped] + [from_other_core(v) for v in own[1:]]


def from_x_ring(hidden, nx):
    return jnp.concatenate([hidden] + [along_x(hidden, j) for j in range(1, nx)], axis=0)


def body(tokens, gain_first, up_first, down_first, gain_second, up_second, down_second):
    ny, nx, nz = lax.axis_size("y"), lax.axis_size("x"), lax.axis_size("z")
    count, channels = tokens.shape
    width = channels * ny * nx
    half = count // 2
    per_y = half // ny
    few = per_y // nx
    hid = 2 * up_first.shape[1]
    wide = hid + LANES
    blocks = 2 * ny

    def held(w, more=0):
        return [pltpu.VMEM((blocks, *w.shape), BF), pltpu.SemaphoreType.DMA((blocks + more,))]

    activate = call(functools.partial(activate_kernel, width=width), sds((few, hid)))
    down_out = sds((nz, per_y, LANES))

    block = pltpu.VMEM(up_first.shape, BF)
    row = pltpu.VMEM((1, channels), F32)
    payload, scaled, kept = call(
        up_own_kernel,
        (sds((half, wide)), sds((half, channels)), sds((per_y + 8, LANES), F32)),
        [
            pltpu.VMEM((half, channels), BF),
            row,
            row,
            pltpu.VMEM((per_y, channels), BF),
            pltpu.VMEM((nx, few, LANES), F32),
            block,
            pltpu.SemaphoreType.DMA((5,)),
        ],
        whole=0,
    )(tokens, gain_first[None, :], gain_second[None, :], up_first)
    payload = call(
        up_other_kernel,
        sds((half, wide)),
        [block, pltpu.VMEM((half, hid // 2), BF), pltpu.SemaphoreType.DMA((1,))],
        whole=1,
        update=2,
    )(scaled, from_other_core(up_first), payload)
    parts = exchange(payload.reshape(ny * nx, few, wide), RA)
    kept = by_plane(kept, lambda z: z // 2)
    swapped, order = [], payload
    for w in (down_second, up_second, down_first):
        w, order = after(w, order)
        order = from_other_core(w)
        swapped.append(order)
    down_first, order = after(down_first, order)
    downs = around(down_first, order, forward=True)
    hidden = activate(parts)

    hidden = from_x_ring(hidden, nx)
    branch = call(down_kernel, down_out, held(down_first, 2), whole=1)(hidden, *downs)
    ups = around(up_second, swapped[1])
    branch = exchange(branch, "z")
    downs = around(down_second, swapped[0])
    middle, payload = call(finish_first_kernel, (sds((per_y, LANES)), sds((nz, per_y + 8, LANES))))(
        branch, kept
    )
    payload = exchange(payload, "z")
    parts = call(up_second_kernel, (sds((few, wide)),) * nx, held(up_second), whole=1)(payload, *ups)
    parts = [parts[0]] + [along_x(parts[j], nx - j) for j in range(1, nx)]
    hidden = activate(*parts)
    hidden = from_x_ring(hidden, nx)
    branch = call(down_kernel, down_out, held(down_second), whole=1)(hidden, *downs)
    finished = call(finish_second_kernel, sds((per_y, LANES)))(exchange(branch, "z"), middle)
    rows = exchange(spread(by_plane(finished, lambda z: -(z // 2)), nz), "z")
    placed = pltpu.VMEM((2 * ny * nx, few, channels), F32)
    return call(assemble_kernel, sds((count, channels)), [placed])(rows, from_other_core(rows))


def solution(mesh):
    fine = Mesh(mesh.devices.reshape(4, 4, 8, 2), ("y", "x", "z", "c"))
    cb = ("z", "c")
    placed = (
        P(None, RA),
        P(RA),
        P(RA, cb),
        P(cb, RA),
        P(RA),
        P(RA, cb),
        P(cb, RA),
    )

    return jax.shard_map(body, mesh=fine, in_specs=placed, out_specs=P(None, RA), check_vma=False)
```

```python
import functools

import jax
import jax.numpy as jnp
from jax import lax
from jax.experimental import pallas as pl
from jax.experimental.pallas import tpu as pltpu
from jax.sharding import Mesh, PartitionSpec as P


RA = ("y", "x")
BF = jnp.bfloat16
F32 = jnp.float32
LANES = 128
EPS = 1e-06


def exchange(parts, axis):
    return lax.all_to_all(parts, axis, 0, 0, tiled=True)


def from_other_core(w):
    return lax.ppermute(w, "c", [(0, 1), (1, 0)])


def along_y(a, shift):
    n = lax.axis_size("y")
    return lax.ppermute(a, "y", [(i, (i + shift) % n) for i in range(n)])


def along_x(a, shift):
    n = lax.axis_size("x")
    return lax.ppermute(a, "x", [(i, (i + shift) % n) for i in range(n)])


def by_plane(a, steps):
    ny, nz = lax.axis_size("y"), lax.axis_size("z")
    perm = [(y * nz + z, (y + steps(z)) % ny * nz + z) for y in range(ny) for z in range(nz)]
    return lax.ppermute(a, ("y", "z"), perm)


def call(kernel, out, scratch=(), limit=16, whole=None, update=None):
    vmem = pl.BlockSpec(memory_space=pltpu.VMEM)
    lies = pl.BlockSpec(memory_space=pltpu.HBM if update is None else pl.ANY)

    def run(*args):
        first = len(args) if whole is None else whole
        if update is None:
            args = [*args[:first], *(pltpu.with_memory_space_constraint(a, pltpu.HBM) for a in args[first:])]
        return pl.pallas_call(
            kernel,
            out_shape=out,
            in_specs=[vmem] * first + [lies] * (len(args) - first),
            out_specs=jax.tree.map(lambda _: vmem if update is None else lies, out),
            scratch_shapes=list(scratch),
            input_output_aliases={} if update is None else {update: 0},
            compiler_params=pltpu.CompilerParams(vmem_limit_bytes=limit << 20),
        )(*args)

    return run


def sds(shape, dtype=BF):
    return jax.ShapeDtypeStruct(shape, dtype)


def stat_columns(sq):
    high = sq.astype(BF)
    low = (sq - high.astype(F32)).astype(BF)
    lane = lax.broadcasted_iota(jnp.int32, (sq.shape[0], LANES), 1)
    block = jnp.where(lane == 0, high.astype(F32), jnp.where(lane == 1, low.astype(F32), 0.0))
    return block.astype(BF)


def fetch(pairs, sems):
    copies = [pltpu.make_async_copy(source, held, sems.at[i]) for i, (source, held) in enumerate(pairs)]
    for copy in copies:
        copy.start()
    return copies


def up_own_kernel(tokens, gain, next_gain, own, out, scaled, kept, x, g, g2, some, some_f, w, sems):
    half, hid = x.shape[0], own.shape[1]
    rows = some.shape[0]
    nx, few, _ = some_f.shape
    y, z, c = lax.axis_index("y"), lax.axis_index("z"), lax.axis_index("c")
    first = pl.multiple_of(c * half, half)
    there = lax.rem(y + z // 2, lax.axis_size("y"))
    copies = fetch(
        (
            (gain, g),
            (tokens.at[pl.ds(first, half), :], x),
            (own, w),
            (tokens.at[pl.ds(pl.multiple_of(first + there * rows, rows), rows), :], some),
            (next_gain, g2),
        ),
        sems,
    )
    copies[0].wait()
    copies[1].wait()
    xf = x[...].astype(F32)
    out[:, 2 * hid :] = stat_columns(jnp.sum(xf * xf, axis=1, keepdims=True))
    scaled[...] = (xf * g[...]).astype(BF)
    copies[2].wait()
    out[:, :hid] = jnp.dot(scaled[...], w[...], preferred_element_type=F32).astype(BF)
    copies[3].wait()
    copies[4].wait()
    left = lax.rem(z, 2) == 0
    chosen = jnp.where(left, some[:, :LANES].astype(F32), some[:, LANES:].astype(F32))
    for i in range(nx):
        some_f[i] = chosen[i * few : (i + 1) * few]
    for j in range(nx):
        kept[j * few : (j + 1) * few, :] = some_f[lax.rem(lax.axis_index("x") + nx - j, nx)]
    chosen = jnp.where(left, g2[:, :LANES], g2[:, LANES:])
    kept[rows:, :] = jnp.broadcast_to(chosen, (8, LANES))


def up_other_kernel(scaled, other, so_far, out, w, part, sems):
    del so_far
    hid = other.shape[1]
    fetch(((other, w),), sems)[0].wait()
    part[...] = jnp.dot(scaled[...], w[...], preferred_element_type=F32).astype(BF)
    fetch(((part, out.at[:, hid : 2 * hid]),), sems)[0].wait()


def summed(parts):
    total = parts[0][...].astype(F32)
    for i in range(1, len(parts) if isinstance(parts, list) else parts.shape[0]):
        total += parts[i][...].astype(F32)
    return total


def activate_kernel(*refs, width):
    *parts, out = refs
    hid = out.shape[1]
    total = summed(parts[0] if len(parts) == 1 else parts)
    meansq = (total[:, hid : hid + 1] + total[:, hid + 1 : hid + 2]) / width
    act = jnp.maximum(total[:, :hid] * lax.rsqrt(meansq + EPS), 0.0)
    out[...] = (act * act).astype(BF)


def arriving(blocks, held, sems, order):
    n, per = held.shape[0] // 2, len(blocks) // 2
    far = n // 2
    pairs, spans = [], {}
    for side, d in order:
        mine = blocks[side * per : (side + 1) * per]
        spot = held.at[side * n + d]
        first = len(pairs)
        if d == far:
            rows = mine[far].shape[0]
            pairs += [(mine[far], spot.at[:rows]), (mine[far + 1], spot.at[rows:])]
        else:
            pairs.append((mine[d + (d > far)], spot))
        spans[side, d] = range(first, len(pairs))
    copies = fetch(pairs, sems)

    def ready(side, d):
        for i in spans[side, d]:
            copies[i].wait()
        return held[side * n + d]

    return ready


def down_kernel(hidden, *refs):
    *blocks, out, held, sems = refs
    n, k = held.shape[0] // 2, held.shape[1]
    ready = arriving(blocks, held, sems, [(side, d) for d in range(n) for side in range(2)])
    for d in range(n):
        acc = jnp.dot(hidden[:, :k], ready(0, d), preferred_element_type=F32)
        acc += jnp.dot(hidden[:, k:], ready(1, d), preferred_element_type=F32)
        acc = acc.astype(BF)
        out[2 * d] = acc[:, :LANES]
        out[2 * d + 1] = acc[:, LANES:]


def finish_first_kernel(parts, kept, mid, payload):
    rows = mid.shape[0]
    x = (0.5 * kept[:rows, :] + summed(parts)).astype(BF)
    gain = kept[rows:, :]
    high = gain.astype(BF).astype(F32)
    rest = gain - high
    middle = rest.astype(BF).astype(F32)
    low = rest - middle
    row = lax.broadcasted_iota(jnp.int32, gain.shape, 0)
    coded = jnp.where(row == 0, high, jnp.where(row == 1, middle, low)).astype(BF)
    mid[...] = x
    for i in range(payload.shape[0]):
        payload[i, :rows, :] = x
        payload[i, rows:, :] = coded


def up_second_kernel(x, *refs):
    *refs, held, sems = refs
    blocks, outs = refs[: held.shape[0] + 2], refs[held.shape[0] + 2 :]
    n, depth, hid = held.shape[0] // 2, *held.shape[1:]
    ready = arriving(blocks, held, sems, [(side, d) for side in range(2) for d in range(n)])
    few = outs[0].shape[0]
    rows = few * len(outs)
    scaled, sq = [], jnp.zeros((rows, 1), F32)
    for i in range(x.shape[0]):
        xf = x[i, :rows, :].astype(F32)
        coded = x[i, rows:, :].astype(F32)
        gain = coded[0:1] + coded[1:2] + coded[2:3]
        sq += jnp.sum(xf * xf, axis=1, keepdims=True)
        scaled.append((xf * gain).astype(BF))
    scaled = jnp.concatenate(scaled, axis=1)
    for side in range(2):
        acc = jnp.zeros((rows, hid), F32)
        for d in range(n):
            acc += jnp.dot(
                scaled[:, d * depth : (d + 1) * depth], ready(side, d), preferred_element_type=F32
            )
        for j, out in enumerate(outs):
            out[:, side * hid : (side + 1) * hid] = acc[j * few : (j + 1) * few].astype(BF)
    for j, out in enumerate(outs):
        out[:, 2 * hid :] = stat_columns(sq[j * few : (j + 1) * few])


def finish_second_kernel(parts, kept, out):
    out[...] = (0.5 * kept[...].astype(F32) + summed(parts)).astype(BF)


def assemble_kernel(own, other, out, placed):
    chunks = own.shape[0]
    ny = chunks // 2
    few = placed.shape[1]
    nx = own.shape[1] // few
    x, y, c = lax.axis_index("x"), lax.axis_index("y"), lax.axis_index("c")
    for side, ref in ((c, own), (1 - c, other)):
        for i in range(chunks):
            block = ref[i].astype(F32)
            row = (side * ny + lax.rem(y + i // 2, ny)) * nx
            column = (i % 2) * LANES
            for j in range(nx):
                placed[row + lax.rem(x + nx - j, nx), :, column : column + LANES] = block[j * few : (j + 1) * few]
    out[...] = placed[...].reshape(out.shape).astype(BF)


def spread(x, peers):
    return jnp.broadcast_to(x[None], (peers, *x.shape))


def around(w, swapped):
    n = lax.axis_size("y")
    half = w.shape[0] // 2
    near = [along_y(w, 1), along_y(w, n - 1)]
    far = [along_y(near[0][:half], 1), along_y(near[1][half:], n - 1)]
    moved = [near[0], *far, near[1]]
    return [w, *moved, swapped] + [from_other_core(v) for v in moved]


def from_x_ring(hidden, nx):
    return jnp.concatenate([hidden] + [along_x(hidden, j) for j in range(1, nx)], axis=0)


def body(tokens, gain_first, up_first, down_first, gain_second, up_second, down_second):
    ny, nx, nz = lax.axis_size("y"), lax.axis_size("x"), lax.axis_size("z")
    count, channels = tokens.shape
    width = channels * ny * nx
    half = count // 2
    per_y = half // ny
    few = per_y // nx
    hid = 2 * up_first.shape[1]
    wide = hid + LANES
    blocks = 2 * ny

    def held(w):
        return [pltpu.VMEM((blocks, *w.shape), BF), pltpu.SemaphoreType.DMA((blocks + 2,))]

    activate = call(functools.partial(activate_kernel, width=width), sds((few, hid)))
    down_out = sds((nz, per_y, LANES))

    block = pltpu.VMEM(up_first.shape, BF)
    row = pltpu.VMEM((1, channels), F32)
    payload, scaled, kept = call(
        up_own_kernel,
        (sds((half, wide)), sds((half, channels)), sds((per_y + 8, LANES), F32)),
        [
            pltpu.VMEM((half, channels), BF),
            row,
            row,
            pltpu.VMEM((per_y, channels), BF),
            pltpu.VMEM((nx, few, LANES), F32),
            block,
            pltpu.SemaphoreType.DMA((5,)),
        ],
        whole=0,
    )(tokens, gain_first[None, :], gain_second[None, :], up_first)
    payload = call(
        up_other_kernel,
        sds((half, wide)),
        [block, pltpu.VMEM((half, hid // 2), BF), pltpu.SemaphoreType.DMA((1,))],
        whole=1,
        update=2,
    )(scaled, from_other_core(up_first), payload)
    parts = exchange(payload.reshape(ny * nx, few, wide), RA)
    kept = by_plane(kept, lambda z: z // 2)
    swapped = [from_other_core(w) for w in (down_first, up_second, down_second)]
    downs = around(down_first, swapped[0])
    hidden = activate(parts)

    hidden = from_x_ring(hidden, nx)
    branch = call(down_kernel, down_out, held(down_first), whole=1)(hidden, *downs)
    ups = around(up_second, swapped[1])
    branch = exchange(branch, "z")
    downs = around(down_second, swapped[2])
    middle, payload = call(finish_first_kernel, (sds((per_y, LANES)), sds((nz, per_y + 8, LANES))))(
        branch, kept
    )
    payload = exchange(payload, "z")
    parts = call(up_second_kernel, (sds((few, wide)),) * nx, held(up_second), whole=1)(payload, *ups)
    parts = [parts[0]] + [along_x(parts[j], nx - j) for j in range(1, nx)]
    hidden = activate(*parts)
    hidden = from_x_ring(hidden, nx)
    branch = call(down_kernel, down_out, held(down_second), whole=1)(hidden, *downs)
    finished = call(finish_second_kernel, sds((per_y, LANES)))(exchange(branch, "z"), middle)
    rows = exchange(spread(by_plane(finished, lambda z: -(z // 2)), nz), "z")
    placed = pltpu.VMEM((2 * ny * nx, few, channels), F32)
    return call(assemble_kernel, sds((count, channels)), [placed])(rows, from_other_core(rows))


def solution(mesh):
    fine = Mesh(mesh.devices.reshape(4, 4, 8, 2), ("y", "x", "z", "c"))
    cb = ("z", "c")
    placed = (
        P(None, RA),
        P(RA),
        P(RA, cb),
        P(cb, RA),
        P(RA),
        P(RA, cb),
        P(cb, RA),
    )

    return jax.shard_map(body, mesh=fine, in_specs=placed, out_specs=P(None, RA), check_vma=False)
```

```python
import functools

import jax
import jax.numpy as jnp
from jax import lax
from jax.experimental import pallas as pl
from jax.experimental.pallas import tpu as pltpu
from jax.sharding import Mesh, PartitionSpec as P


RA = ("y", "x")
BF = jnp.bfloat16
F32 = jnp.float32
LANES = 128
EPS = 1e-06


def exchange(parts, axis):
    return lax.all_to_all(parts, axis, 0, 0, tiled=True)


def from_other_core(w):
    return lax.ppermute(w, "c", [(0, 1), (1, 0)])


def along_y(a, shift):
    n = lax.axis_size("y")
    return lax.ppermute(a, "y", [(i, (i + shift) % n) for i in range(n)])


def along_x(a, shift):
    n = lax.axis_size("x")
    return lax.ppermute(a, "x", [(i, (i + shift) % n) for i in range(n)])


def by_plane(a, steps):
    ny, nz = lax.axis_size("y"), lax.axis_size("z")
    perm = [(y * nz + z, (y + steps(z)) % ny * nz + z) for y in range(ny) for z in range(nz)]
    return lax.ppermute(a, ("y", "z"), perm)


def call(kernel, out, scratch=(), limit=16, whole=None, update=None):
    vmem = pl.BlockSpec(memory_space=pltpu.VMEM)
    lies = pl.BlockSpec(memory_space=pltpu.HBM if update is None else pl.ANY)

    def run(*args):
        first = len(args) if whole is None else whole
        if update is None:
            args = [*args[:first], *(pltpu.with_memory_space_constraint(a, pltpu.HBM) for a in args[first:])]
        return pl.pallas_call(
            kernel,
            out_shape=out,
            in_specs=[vmem] * first + [lies] * (len(args) - first),
            out_specs=jax.tree.map(lambda _: vmem if update is None else lies, out),
            scratch_shapes=list(scratch),
            input_output_aliases={} if update is None else {update: 0},
            compiler_params=pltpu.CompilerParams(vmem_limit_bytes=limit << 20),
        )(*args)

    return run


def sds(shape, dtype=BF):
    return jax.ShapeDtypeStruct(shape, dtype)


def stat_columns(sq):
    high = sq.astype(BF)
    low = (sq - high.astype(F32)).astype(BF)
    lane = lax.broadcasted_iota(jnp.int32, (sq.shape[0], LANES), 1)
    block = jnp.where(lane == 0, high.astype(F32), jnp.where(lane == 1, low.astype(F32), 0.0))
    return block.astype(BF)


def fetch(pairs, sems):
    copies = [pltpu.make_async_copy(source, held, sems.at[i]) for i, (source, held) in enumerate(pairs)]
    for copy in copies:
        copy.start()
    return copies


def up_own_kernel(tokens, gain, next_gain, own, out, scaled, kept, x, g, g2, some, some_f, w, sems):
    half, hid = x.shape[0], own.shape[1]
    rows = some.shape[0]
    nx, few, _ = some_f.shape
    y, z, c = lax.axis_index("y"), lax.axis_index("z"), lax.axis_index("c")
    first = pl.multiple_of(c * half, half)
    there = lax.rem(y + z // 2, lax.axis_size("y"))
    copies = fetch(
        (
            (gain, g),
            (tokens.at[pl.ds(first, half), :], x),
            (own, w),
            (tokens.at[pl.ds(pl.multiple_of(first + there * rows, rows), rows), :], some),
            (next_gain, g2),
        ),
        sems,
    )
    copies[0].wait()
    copies[1].wait()
    xf = x[...].astype(F32)
    out[:, 2 * hid :] = stat_columns(jnp.sum(xf * xf, axis=1, keepdims=True))
    scaled[...] = (xf * g[...]).astype(BF)
    copies[2].wait()
    out[:, :hid] = jnp.dot(scaled[...], w[...], preferred_element_type=F32).astype(BF)
    copies[3].wait()
    copies[4].wait()
    left = lax.rem(z, 2) == 0
    chosen = jnp.where(left, some[:, :LANES].astype(F32), some[:, LANES:].astype(F32))
    for i in range(nx):
        some_f[i] = chosen[i * few : (i + 1) * few]
    for j in range(nx):
        kept[j * few : (j + 1) * few, :] = some_f[lax.rem(lax.axis_index("x") + nx - j, nx)]
    chosen = jnp.where(left, g2[:, :LANES], g2[:, LANES:])
    kept[rows:, :] = jnp.broadcast_to(chosen, (8, LANES))


def up_other_kernel(scaled, other, so_far, out, w, part, sems):
    del so_far
    hid = other.shape[1]
    fetch(((other, w),), sems)[0].wait()
    part[...] = jnp.dot(scaled[...], w[...], preferred_element_type=F32).astype(BF)
    fetch(((part, out.at[:, hid : 2 * hid]),), sems)[0].wait()


def summed(parts):
    total = parts[0][...].astype(F32)
    for i in range(1, len(parts) if isinstance(parts, list) else parts.shape[0]):
        total += parts[i][...].astype(F32)
    return total


def activate_kernel(*refs, width):
    *parts, out = refs
    hid = out.shape[1]
    total = summed(parts[0] if len(parts) == 1 else parts)
    meansq = (total[:, hid : hid + 1] + total[:, hid + 1 : hid + 2]) / width
    act = jnp.maximum(total[:, :hid] * lax.rsqrt(meansq + EPS), 0.0)
    out[...] = (act * act).astype(BF)


def arriving(blocks, held, sems, order):
    n, per = held.shape[0] // 2, len(blocks) // 2
    far = n // 2
    pairs, spans = [], {}
    for side, d in order:
        mine = blocks[side * per : (side + 1) * per]
        spot = held.at[side * n + d]
        first = len(pairs)
        if d == far:
            rows = mine[far].shape[0]
            pairs += [(mine[far], spot.at[:rows]), (mine[far + 1], spot.at[rows:])]
        else:
            pairs.append((mine[d + (d > far)], spot))
        spans[side, d] = range(first, len(pairs))
    copies = fetch(pairs, sems)

    def ready(side, d):
        for i in spans[side, d]:
            copies[i].wait()
        return held[side * n + d]

    return ready


def down_kernel(hidden, *refs):
    *blocks, out, held, sems = refs
    n, k = held.shape[0] // 2, held.shape[1]
    ready = arriving(blocks, held, sems, [(side, d) for d in range(n) for side in range(2)])
    for d in range(n):
        acc = jnp.dot(hidden[:, :k], ready(0, d), preferred_element_type=F32)
        acc += jnp.dot(hidden[:, k:], ready(1, d), preferred_element_type=F32)
        acc = acc.astype(BF)
        out[2 * d] = acc[:, :LANES]
        out[2 * d + 1] = acc[:, LANES:]


def finish_first_kernel(parts, kept, mid, payload):
    rows = mid.shape[0]
    x = (0.5 * kept[:rows, :] + summed(parts)).astype(BF)
    gain = kept[rows:, :]
    high = gain.astype(BF).astype(F32)
    rest = gain - high
    middle = rest.astype(BF).astype(F32)
    low = rest - middle
    row = lax.broadcasted_iota(jnp.int32, gain.shape, 0)
    coded = jnp.where(row == 0, high, jnp.where(row == 1, middle, low)).astype(BF)
    mid[...] = x
    for i in range(payload.shape[0]):
        payload[i, :rows, :] = x
        payload[i, rows:, :] = coded


def up_second_kernel(x, *refs):
    *refs, held, sems = refs
    blocks, outs = refs[: held.shape[0] + 2], refs[held.shape[0] + 2 :]
    n, depth, hid = held.shape[0] // 2, *held.shape[1:]
    ready = arriving(blocks, held, sems, [(side, d) for side in range(2) for d in range(n)])
    few = outs[0].shape[0]
    rows = few * len(outs)
    scaled, sq = [], jnp.zeros((rows, 1), F32)
    for i in range(x.shape[0]):
        xf = x[i, :rows, :].astype(F32)
        coded = x[i, rows:, :].astype(F32)
        gain = coded[0:1] + coded[1:2] + coded[2:3]
        sq += jnp.sum(xf * xf, axis=1, keepdims=True)
        scaled.append((xf * gain).astype(BF))
    scaled = jnp.concatenate(scaled, axis=1)
    for side in range(2):
        acc = jnp.zeros((rows, hid), F32)
        for d in range(n):
            acc += jnp.dot(
                scaled[:, d * depth : (d + 1) * depth], ready(side, d), preferred_element_type=F32
            )
        for j, out in enumerate(outs):
            out[:, side * hid : (side + 1) * hid] = acc[j * few : (j + 1) * few].astype(BF)
    for j, out in enumerate(outs):
        out[:, 2 * hid :] = stat_columns(sq[j * few : (j + 1) * few])


def finish_second_kernel(parts, kept, out):
    out[...] = (0.5 * kept[...].astype(F32) + summed(parts)).astype(BF)


def assemble_kernel(own, other, out, placed):
    chunks = own.shape[0]
    ny = chunks // 2
    few = placed.shape[1]
    nx = own.shape[1] // few
    x, y, c = lax.axis_index("x"), lax.axis_index("y"), lax.axis_index("c")
    for side, ref in ((c, own), (1 - c, other)):
        for i in range(chunks):
            block = ref[i].astype(F32)
            row = (side * ny + lax.rem(y + i // 2, ny)) * nx
            column = (i % 2) * LANES
            for j in range(nx):
                placed[row + lax.rem(x + nx - j, nx), :, column : column + LANES] = block[j * few : (j + 1) * few]
    out[...] = placed[...].reshape(out.shape).astype(BF)


def spread(x, peers):
    return jnp.broadcast_to(x[None], (peers, *x.shape))


def around(w, swapped):
    n = lax.axis_size("y")
    half = w.shape[0] // 2
    near = [along_y(w, 1), along_y(w, n - 1)]
    far = [along_y(near[0][:half], 1), along_y(near[1][half:], n - 1)]
    moved = [near[0], *far, near[1]]
    return [w, *moved, swapped] + [from_other_core(v) for v in moved]


def from_x_ring(hidden, nx):
    return jnp.concatenate([hidden] + [along_x(hidden, j) for j in range(1, nx)], axis=0)


def body(tokens, gain_first, up_first, down_first, gain_second, up_second, down_second):
    ny, nx, nz = lax.axis_size("y"), lax.axis_size("x"), lax.axis_size("z")
    count, channels = tokens.shape
    width = channels * ny * nx
    half = count // 2
    per_y = half // ny
    few = per_y // nx
    hid = 2 * up_first.shape[1]
    wide = hid + LANES
    blocks = 2 * ny

    def held(w):
        return [pltpu.VMEM((blocks, *w.shape), BF), pltpu.SemaphoreType.DMA((blocks + 2,))]

    activate = call(functools.partial(activate_kernel, width=width), sds((few, hid)))
    down_out = sds((nz, per_y, LANES))

    block = pltpu.VMEM(up_first.shape, BF)
    row = pltpu.VMEM((1, channels), F32)
    up_own = call(
        up_own_kernel,
        (sds((half, wide)), sds((half, channels)), sds((per_y + 8, LANES), F32)),
        [
            pltpu.VMEM((half, channels), BF),
            row,
            row,
            pltpu.VMEM((per_y, channels), BF),
            pltpu.VMEM((nx, few, LANES), F32),
            block,
            pltpu.SemaphoreType.DMA((5,)),
        ],
        whole=0,
    )
    payload, scaled, kept = up_own(tokens, gain_first[None, :], gain_second[None, :], up_first)
    payload = call(
        up_other_kernel,
        sds((half, wide)),
        [block, pltpu.VMEM((half, hid // 2), BF), pltpu.SemaphoreType.DMA((1,))],
        whole=1,
        update=2,
    )(scaled, from_other_core(up_first), payload)
    parts = exchange(payload.reshape(ny * nx, few, wide), RA)
    kept = by_plane(kept, lambda z: z // 2)
    swapped = [from_other_core(w) for w in (down_first, up_second, down_second)]
    downs = around(down_first, swapped[0])
    hidden = activate(parts)

    hidden = from_x_ring(hidden, nx)
    branch = call(down_kernel, down_out, held(down_first), whole=1)(hidden, *downs)
    ups = around(up_second, swapped[1])
    branch = exchange(branch, "z")
    downs = around(down_second, swapped[2])
    middle, payload = call(finish_first_kernel, (sds((per_y, LANES)), sds((nz, per_y + 8, LANES))))(
        branch, kept
    )
    payload = exchange(payload, "z")
    parts = call(up_second_kernel, (sds((few, wide)),) * nx, held(up_second), whole=1)(payload, *ups)
    parts = [parts[0]] + [along_x(parts[j], nx - j) for j in range(1, nx)]
    hidden = activate(*parts)
    hidden = from_x_ring(hidden, nx)
    branch = call(down_kernel, down_out, held(down_second), whole=1)(hidden, *downs)
    finished = call(finish_second_kernel, sds((per_y, LANES)))(exchange(branch, "z"), middle)
    rows = exchange(spread(by_plane(finished, lambda z: -(z // 2)), nz), "z")
    placed = pltpu.VMEM((2 * ny * nx, few, channels), F32)
    return call(assemble_kernel, sds((count, channels)), [placed])(rows, from_other_core(rows))


def solution(mesh):
    fine = Mesh(mesh.devices.reshape(4, 4, 8, 2), ("y", "x", "z", "c"))
    cb = ("z", "c")
    placed = (
        P(None, RA),
        P(RA),
        P(RA, cb),
        P(cb, RA),
        P(RA),
        P(RA, cb),
        P(cb, RA),
    )

    return jax.shard_map(body, mesh=fine, in_specs=placed, out_specs=P(None, RA), check_vma=False)
```

```python
import functools

import jax
import jax.numpy as jnp
from jax import lax
from jax.experimental import pallas as pl
from jax.experimental.pallas import tpu as pltpu
from jax.sharding import Mesh, PartitionSpec as P


RA = ("y", "x")
BF = jnp.bfloat16
F32 = jnp.float32
LANES = 128
EPS = 1e-06


def exchange(parts, axis):
    return lax.all_to_all(parts, axis, 0, 0, tiled=True)


def from_other_core(w):
    return lax.ppermute(w, "c", [(0, 1), (1, 0)])


def along_y(a, shift):
    n = lax.axis_size("y")
    return lax.ppermute(a, "y", [(i, (i + shift) % n) for i in range(n)])


def along_x(a, shift):
    n = lax.axis_size("x")
    return lax.ppermute(a, "x", [(i, (i + shift) % n) for i in range(n)])


def by_plane(a, steps):
    ny, nz = lax.axis_size("y"), lax.axis_size("z")
    perm = [(y * nz + z, (y + steps(z)) % ny * nz + z) for y in range(ny) for z in range(nz)]
    return lax.ppermute(a, ("y", "z"), perm)


def call(kernel, out, scratch=(), limit=16, whole=None, update=None):
    vmem = pl.BlockSpec(memory_space=pltpu.VMEM)
    lies = pl.BlockSpec(memory_space=pltpu.HBM if update is None else pl.ANY)

    def run(*args):
        first = len(args) if whole is None else whole
        if update is None:
            args = [*args[:first], *(pltpu.with_memory_space_constraint(a, pltpu.HBM) for a in args[first:])]
        return pl.pallas_call(
            kernel,
            out_shape=out,
            in_specs=[vmem] * first + [lies] * (len(args) - first),
            out_specs=jax.tree.map(lambda _: vmem if update is None else lies, out),
            scratch_shapes=list(scratch),
            input_output_aliases={} if update is None else {update: 0},
            compiler_params=pltpu.CompilerParams(vmem_limit_bytes=limit << 20),
        )(*args)

    return run


def sds(shape, dtype=BF):
    return jax.ShapeDtypeStruct(shape, dtype)


def stat_columns(sq):
    high = sq.astype(BF)
    low = (sq - high.astype(F32)).astype(BF)
    lane = lax.broadcasted_iota(jnp.int32, (sq.shape[0], LANES), 1)
    block = jnp.where(lane == 0, high.astype(F32), jnp.where(lane == 1, low.astype(F32), 0.0))
    return block.astype(BF)


def fetch(pairs, sems):
    copies = [pltpu.make_async_copy(source, held, sems.at[i]) for i, (source, held) in enumerate(pairs)]
    for copy in copies:
        copy.start()
    return copies


def up_own_kernel(tokens, gain, next_gain, own, out, scaled, kept, x, g, g2, some, some_f, w, sems):
    half, hid = x.shape[0], own.shape[1]
    rows = some.shape[0]
    nx, few, _ = some_f.shape
    y, z, c = lax.axis_index("y"), lax.axis_index("z"), lax.axis_index("c")
    first = pl.multiple_of(c * half, half)
    there = lax.rem(y + z // 2, lax.axis_size("y"))
    copies = fetch(
        (
            (gain, g),
            (tokens.at[pl.ds(first, half), :], x),
            (own, w),
            (tokens.at[pl.ds(pl.multiple_of(first + there * rows, rows), rows), :], some),
            (next_gain, g2),
        ),
        sems,
    )
    copies[0].wait()
    copies[1].wait()
    xf = x[...].astype(F32)
    out[:, 2 * hid :] = stat_columns(jnp.sum(xf * xf, axis=1, keepdims=True))
    scaled[...] = (xf * g[...]).astype(BF)
    copies[2].wait()
    out[:, :hid] = jnp.dot(scaled[...], w[...], preferred_element_type=F32).astype(BF)
    copies[3].wait()
    copies[4].wait()
    left = lax.rem(z, 2) == 0
    chosen = jnp.where(left, some[:, :LANES].astype(F32), some[:, LANES:].astype(F32))
    for i in range(nx):
        some_f[i] = chosen[i * few : (i + 1) * few]
    for j in range(nx):
        kept[j * few : (j + 1) * few, :] = some_f[lax.rem(lax.axis_index("x") + nx - j, nx)]
    chosen = jnp.where(left, g2[:, :LANES], g2[:, LANES:])
    kept[rows:, :] = jnp.broadcast_to(chosen, (8, LANES))


def up_other_kernel(scaled, other, so_far, out, w, part, sems):
    del so_far
    hid = other.shape[1]
    fetch(((other, w),), sems)[0].wait()
    part[...] = jnp.dot(scaled[...], w[...], preferred_element_type=F32).astype(BF)
    fetch(((part, out.at[:, hid : 2 * hid]),), sems)[0].wait()


def summed(parts):
    total = parts[0][...].astype(F32)
    for i in range(1, len(parts) if isinstance(parts, list) else parts.shape[0]):
        total += parts[i][...].astype(F32)
    return total


def activate_kernel(*refs, width):
    *parts, out = refs
    hid = out.shape[1]
    total = summed(parts[0] if len(parts) == 1 else parts)
    meansq = (total[:, hid : hid + 1] + total[:, hid + 1 : hid + 2]) / width
    act = jnp.maximum(total[:, :hid] * lax.rsqrt(meansq + EPS), 0.0)
    out[...] = (act * act).astype(BF)


def arriving(blocks, held, sems, order):
    n, per = held.shape[0] // 2, len(blocks) // 2
    far = n // 2
    pairs, spans = [], {}
    for side, d in order:
        mine = blocks[side * per : (side + 1) * per]
        spot = held.at[side * n + d]
        first = len(pairs)
        if d == far:
            rows = mine[far].shape[0]
            pairs += [(mine[far], spot.at[:rows]), (mine[far + 1], spot.at[rows:])]
        else:
            pairs.append((mine[d + (d > far)], spot))
        spans[side, d] = range(first, len(pairs))
    copies = fetch(pairs, sems)

    def ready(side, d):
        for i in spans[side, d]:
            copies[i].wait()
        return held[side * n + d]

    return ready


def down_kernel(hidden, *refs):
    *blocks, out, held, sems = refs
    n, k = held.shape[0] // 2, held.shape[1]
    ready = arriving(blocks, held, sems, [(side, d) for d in range(n) for side in range(2)])
    for d in range(n):
        acc = jnp.dot(hidden[:, :k], ready(0, d), preferred_element_type=F32)
        acc += jnp.dot(hidden[:, k:], ready(1, d), preferred_element_type=F32)
        acc = acc.astype(BF)
        out[2 * d] = acc[:, :LANES]
        out[2 * d + 1] = acc[:, LANES:]


def finish_first_kernel(parts, kept, mid, payload):
    rows = mid.shape[0]
    x = (0.5 * kept[:rows, :] + summed(parts)).astype(BF)
    gain = kept[rows:, :]
    high = gain.astype(BF).astype(F32)
    rest = gain - high
    middle = rest.astype(BF).astype(F32)
    low = rest - middle
    row = lax.broadcasted_iota(jnp.int32, gain.shape, 0)
    coded = jnp.where(row == 0, high, jnp.where(row == 1, middle, low)).astype(BF)
    mid[...] = x
    for i in range(payload.shape[0]):
        payload[i, :rows, :] = x
        payload[i, rows:, :] = coded


def up_second_kernel(x, *refs):
    *refs, held, sems = refs
    blocks, outs = refs[: held.shape[0] + 2], refs[held.shape[0] + 2 :]
    n, depth, hid = held.shape[0] // 2, *held.shape[1:]
    ready = arriving(blocks, held, sems, [(side, d) for side in range(2) for d in range(n)])
    few = outs[0].shape[0]
    rows = few * len(outs)
    scaled, sq = [], jnp.zeros((rows, 1), F32)
    for i in range(x.shape[0]):
        xf = x[i, :rows, :].astype(F32)
        coded = x[i, rows:, :].astype(F32)
        gain = coded[0:1] + coded[1:2] + coded[2:3]
        sq += jnp.sum(xf * xf, axis=1, keepdims=True)
        scaled.append((xf * gain).astype(BF))
    scaled = jnp.concatenate(scaled, axis=1)
    for side in range(2):
        acc = jnp.zeros((rows, hid), F32)
        for d in range(n):
            acc += jnp.dot(
                scaled[:, d * depth : (d + 1) * depth], ready(side, d), preferred_element_type=F32
            )
        for j, out in enumerate(outs):
            out[:, side * hid : (side + 1) * hid] = acc[j * few : (j + 1) * few].astype(BF)
    for j, out in enumerate(outs):
        out[:, 2 * hid :] = stat_columns(sq[j * few : (j + 1) * few])


def finish_second_kernel(parts, kept, out):
    out[...] = (0.5 * kept[...].astype(F32) + summed(parts)).astype(BF)


def assemble_kernel(own, other, out, placed):
    chunks = own.shape[0]
    ny = chunks // 2
    few = placed.shape[1]
    nx = own.shape[1] // few
    x, y, c = lax.axis_index("x"), lax.axis_index("y"), lax.axis_index("c")
    for side, ref in ((c, own), (1 - c, other)):
        for i in range(chunks):
            block = ref[i].astype(F32)
            row = (side * ny + lax.rem(y + i // 2, ny)) * nx
            column = (i % 2) * LANES
            for j in range(nx):
                placed[row + lax.rem(x + nx - j, nx), :, column : column + LANES] = block[j * few : (j + 1) * few]
    out[...] = placed[...].reshape(out.shape).astype(BF)


def spread(x, peers):
    return jnp.broadcast_to(x[None], (peers, *x.shape))


def around(w, swapped):
    n = lax.axis_size("y")
    half = w.shape[0] // 2
    near = [along_y(w, 1), along_y(w, n - 1)]
    far = [along_y(near[0][:half], 1), along_y(near[1][half:], n - 1)]
    moved = [near[0], *far, near[1]]
    return [w, *moved, swapped] + [from_other_core(v) for v in moved]


def far_first(n):
    return sorted(range(1, n), key=lambda j: -min(j, n - j))


def from_x_ring(hidden, nx):
    moved = {j: along_x(hidden, j) for j in far_first(nx)}
    return jnp.concatenate([hidden] + [moved[j] for j in range(1, nx)], axis=0)


def body(tokens, gain_first, up_first, down_first, gain_second, up_second, down_second):
    ny, nx, nz = lax.axis_size("y"), lax.axis_size("x"), lax.axis_size("z")
    count, channels = tokens.shape
    width = channels * ny * nx
    half = count // 2
    per_y = half // ny
    few = per_y // nx
    hid = 2 * up_first.shape[1]
    wide = hid + LANES
    blocks = 2 * ny

    def held(w):
        return [pltpu.VMEM((blocks, *w.shape), BF), pltpu.SemaphoreType.DMA((blocks + 2,))]

    activate = call(functools.partial(activate_kernel, width=width), sds((few, hid)))
    down_out = sds((nz, per_y, LANES))

    block = pltpu.VMEM(up_first.shape, BF)
    row = pltpu.VMEM((1, channels), F32)
    up_own = call(
        up_own_kernel,
        (sds((half, wide)), sds((half, channels)), sds((per_y + 8, LANES), F32)),
        [
            pltpu.VMEM((half, channels), BF),
            row,
            row,
            pltpu.VMEM((per_y, channels), BF),
            pltpu.VMEM((nx, few, LANES), F32),
            block,
            pltpu.SemaphoreType.DMA((5,)),
        ],
        whole=0,
    )
    payload, scaled, kept = up_own(tokens, gain_first[None, :], gain_second[None, :], up_first)
    payload = call(
        up_other_kernel,
        sds((half, wide)),
        [block, pltpu.VMEM((half, hid // 2), BF), pltpu.SemaphoreType.DMA((1,))],
        whole=1,
        update=2,
    )(scaled, from_other_core(up_first), payload)
    parts = exchange(payload.reshape(ny * nx, few, wide), RA)
    kept = by_plane(kept, lambda z: z // 2)
    swapped = [from_other_core(w) for w in (down_first, up_second, down_second)]
    downs = around(down_first, swapped[0])
    hidden = activate(parts)

    hidden = from_x_ring(hidden, nx)
    branch = call(down_kernel, down_out, held(down_first), whole=1)(hidden, *downs)
    ups = around(up_second, swapped[1])
    branch = exchange(branch, "z")
    downs = around(down_second, swapped[2])
    finish_first = call(finish_first_kernel, (sds((per_y, LANES)), sds((nz, per_y + 8, LANES))))
    middle, payload = finish_first(branch, kept)
    payload = exchange(payload, "z")
    parts = call(up_second_kernel, (sds((few, wide)),) * nx, held(up_second), whole=1)(payload, *ups)
    parts = [parts[0]] + [along_x(parts[j], nx - j) for j in far_first(nx)]
    hidden = activate(*parts)
    hidden = from_x_ring(hidden, nx)
    branch = call(down_kernel, down_out, held(down_second), whole=1)(hidden, *downs)
    finished = call(finish_second_kernel, sds((per_y, LANES)))(exchange(branch, "z"), middle)
    rows = exchange(spread(by_plane(finished, lambda z: -(z // 2)), nz), "z")
    placed = pltpu.VMEM((2 * ny * nx, few, channels), F32)
    return call(assemble_kernel, sds((count, channels)), [placed])(rows, from_other_core(rows))


def solution(mesh):
    fine = Mesh(mesh.devices.reshape(4, 4, 8, 2), ("y", "x", "z", "c"))
    cb = ("z", "c")
    placed = (
        P(None, RA),
        P(RA),
        P(RA, cb),
        P(cb, RA),
        P(RA),
        P(RA, cb),
        P(cb, RA),
    )

    return jax.shard_map(body, mesh=fine, in_specs=placed, out_specs=P(None, RA), check_vma=False)
```

```python
import functools

import jax
import jax.numpy as jnp
from jax import lax
from jax.experimental import pallas as pl
from jax.experimental.pallas import tpu as pltpu
from jax.sharding import Mesh, PartitionSpec as P


RA = ("y", "x")
BF = jnp.bfloat16
F32 = jnp.float32
LANES = 128
EPS = 1e-06


def exchange(parts, axis):
    return lax.all_to_all(parts, axis, 0, 0, tiled=True)


def from_other_core(w):
    return lax.ppermute(w, "c", [(0, 1), (1, 0)])


def along_y(a, shift):
    n = lax.axis_size("y")
    return lax.ppermute(a, "y", [(i, (i + shift) % n) for i in range(n)])


def along_x(a, shift):
    n = lax.axis_size("x")
    return lax.ppermute(a, "x", [(i, (i + shift) % n) for i in range(n)])


def by_plane(a, steps):
    ny, nz = lax.axis_size("y"), lax.axis_size("z")
    perm = [(y * nz + z, (y + steps(z)) % ny * nz + z) for y in range(ny) for z in range(nz)]
    return lax.ppermute(a, ("y", "z"), perm)


def call(kernel, out, scratch=(), limit=16, whole=None, update=None):
    vmem = pl.BlockSpec(memory_space=pltpu.VMEM)
    lies = pl.BlockSpec(memory_space=pltpu.HBM if update is None else pl.ANY)

    def run(*args):
        first = len(args) if whole is None else whole
        if update is None:
            args = [*args[:first], *(pltpu.with_memory_space_constraint(a, pltpu.HBM) for a in args[first:])]
        return pl.pallas_call(
            kernel,
            out_shape=out,
            in_specs=[vmem] * first + [lies] * (len(args) - first),
            out_specs=jax.tree.map(lambda _: vmem if update is None else lies, out),
            scratch_shapes=list(scratch),
            input_output_aliases={} if update is None else {update: 0},
            compiler_params=pltpu.CompilerParams(vmem_limit_bytes=limit << 20),
        )(*args)

    return run


def sds(shape, dtype=BF):
    return jax.ShapeDtypeStruct(shape, dtype)


def stat_columns(sq):
    high = sq.astype(BF)
    low = (sq - high.astype(F32)).astype(BF)
    lane = lax.broadcasted_iota(jnp.int32, (sq.shape[0], LANES), 1)
    block = jnp.where(lane == 0, high.astype(F32), jnp.where(lane == 1, low.astype(F32), 0.0))
    return block.astype(BF)


def fetch(pairs, sems):
    copies = [pltpu.make_async_copy(source, held, sems.at[i]) for i, (source, held) in enumerate(pairs)]
    for copy in copies:
        copy.start()
    return copies


def up_own_kernel(tokens, gain, next_gain, own, out, scaled, kept, x, g, g2, some, some_f, w, sems):
    half, hid = x.shape[0], own.shape[1]
    rows = some.shape[0]
    nx, few, _ = some_f.shape
    y, z, c = lax.axis_index("y"), lax.axis_index("z"), lax.axis_index("c")
    first = pl.multiple_of(c * half, half)
    there = lax.rem(y + z // 2, lax.axis_size("y"))
    copies = fetch(
        (
            (gain, g),
            (tokens.at[pl.ds(first, half), :], x),
            (own, w),
            (tokens.at[pl.ds(pl.multiple_of(first + there * rows, rows), rows), :], some),
            (next_gain, g2),
        ),
        sems,
    )
    copies[0].wait()
    copies[1].wait()
    xf = x[...].astype(F32)
    out[:, 2 * hid :] = stat_columns(jnp.sum(xf * xf, axis=1, keepdims=True))
    scaled[...] = (xf * g[...]).astype(BF)
    copies[2].wait()
    out[:, :hid] = jnp.dot(scaled[...], w[...], preferred_element_type=F32).astype(BF)
    copies[3].wait()
    copies[4].wait()
    left = lax.rem(z, 2) == 0
    chosen = jnp.where(left, some[:, :LANES].astype(F32), some[:, LANES:].astype(F32))
    for i in range(nx):
        some_f[i] = chosen[i * few : (i + 1) * few]
    for j in range(nx):
        kept[j * few : (j + 1) * few, :] = some_f[lax.rem(lax.axis_index("x") + nx - j, nx)]
    chosen = jnp.where(left, g2[:, :LANES], g2[:, LANES:])
    kept[rows:, :] = jnp.broadcast_to(chosen, (8, LANES))


def up_other_kernel(scaled, other, so_far, out, w, part, sems):
    del so_far
    hid = other.shape[1]
    fetch(((other, w),), sems)[0].wait()
    part[...] = jnp.dot(scaled[...], w[...], preferred_element_type=F32).astype(BF)
    fetch(((part, out.at[:, hid : 2 * hid]),), sems)[0].wait()


def summed(parts):
    total = parts[0][...].astype(F32)
    for i in range(1, len(parts) if isinstance(parts, list) else parts.shape[0]):
        total += parts[i][...].astype(F32)
    return total


def activate_kernel(*refs, width):
    *parts, out = refs
    hid = out.shape[1]
    total = summed(parts[0] if len(parts) == 1 else parts)
    meansq = (total[:, hid : hid + 1] + total[:, hid + 1 : hid + 2]) / width
    act = jnp.maximum(total[:, :hid] * lax.rsqrt(meansq + EPS), 0.0)
    out[...] = (act * act).astype(BF)


def arriving(blocks, held, sems, order):
    n, per = held.shape[0] // 2, len(blocks) // 2
    far = n // 2
    pairs, spans = [], {}
    for side, d in order:
        mine = blocks[side * per : (side + 1) * per]
        spot = held.at[side * n + d]
        first = len(pairs)
        if d == far and per > n:
            rows = mine[far].shape[0]
            pairs += [(mine[far], spot.at[:rows]), (mine[far + 1], spot.at[rows:])]
        else:
            pairs.append((mine[d + (d > far) * (per - n)], spot))
        spans[side, d] = range(first, len(pairs))
    copies = fetch(pairs, sems)

    def ready(side, d):
        for i in spans[side, d]:
            copies[i].wait()
        return held[side * n + d]

    return ready


def down_kernel(hidden, *refs):
    *blocks, out, held, sems = refs
    n, k = held.shape[0] // 2, held.shape[1]
    ready = arriving(blocks, held, sems, [(side, d) for d in range(n) for side in range(2)])
    for d in range(n):
        acc = jnp.dot(hidden[:, :k], ready(0, d), preferred_element_type=F32)
        acc += jnp.dot(hidden[:, k:], ready(1, d), preferred_element_type=F32)
        acc = acc.astype(BF)
        out[2 * d] = acc[:, :LANES]
        out[2 * d + 1] = acc[:, LANES:]


def finish_first_kernel(parts, kept, mid, payload):
    rows = mid.shape[0]
    x = (0.5 * kept[:rows, :] + summed(parts)).astype(BF)
    gain = kept[rows:, :]
    high = gain.astype(BF).astype(F32)
    rest = gain - high
    middle = rest.astype(BF).astype(F32)
    low = rest - middle
    row = lax.broadcasted_iota(jnp.int32, gain.shape, 0)
    coded = jnp.where(row == 0, high, jnp.where(row == 1, middle, low)).astype(BF)
    mid[...] = x
    for i in range(payload.shape[0]):
        payload[i, :rows, :] = x
        payload[i, rows:, :] = coded


def up_second_kernel(x, *refs):
    *refs, held, sems = refs
    count = sems.shape[0]
    blocks, outs = refs[:count], refs[count:]
    n, depth, hid = held.shape[0] // 2, *held.shape[1:]
    ready = arriving(blocks, held, sems, [(side, d) for side in range(2) for d in range(n)])
    few = outs[0].shape[0]
    rows = few * len(outs)
    scaled, sq = [], jnp.zeros((rows, 1), F32)
    for i in range(x.shape[0]):
        xf = x[i, :rows, :].astype(F32)
        coded = x[i, rows:, :].astype(F32)
        gain = coded[0:1] + coded[1:2] + coded[2:3]
        sq += jnp.sum(xf * xf, axis=1, keepdims=True)
        scaled.append((xf * gain).astype(BF))
    scaled = jnp.concatenate(scaled, axis=1)
    for side in range(2):
        acc = jnp.zeros((rows, hid), F32)
        for d in range(n):
            acc += jnp.dot(
                scaled[:, d * depth : (d + 1) * depth], ready(side, d), preferred_element_type=F32
            )
        for j, out in enumerate(outs):
            out[:, side * hid : (side + 1) * hid] = acc[j * few : (j + 1) * few].astype(BF)
    for j, out in enumerate(outs):
        out[:, 2 * hid :] = stat_columns(sq[j * few : (j + 1) * few])


def finish_second_kernel(parts, kept, out):
    out[...] = (0.5 * kept[...].astype(F32) + summed(parts)).astype(BF)


def assemble_kernel(own, other, out, placed):
    chunks = own.shape[0]
    ny = chunks // 2
    few = placed.shape[1]
    nx = own.shape[1] // few
    x, y, c = lax.axis_index("x"), lax.axis_index("y"), lax.axis_index("c")
    for side, ref in ((c, own), (1 - c, other)):
        for i in range(chunks):
            block = ref[i].astype(F32)
            row = (side * ny + lax.rem(y + i // 2, ny)) * nx
            column = (i % 2) * LANES
            for j in range(nx):
                placed[row + lax.rem(x + nx - j, nx), :, column : column + LANES] = block[j * few : (j + 1) * few]
    out[...] = placed[...].reshape(out.shape).astype(BF)


def spread(x, peers):
    return jnp.broadcast_to(x[None], (peers, *x.shape))


def around(w, swapped, halves=False):
    n = lax.axis_size("y")
    half = w.shape[0] // 2
    near = [along_y(w, 1), along_y(w, n - 1)]
    if halves:
        far = [along_y(near[0][:half], 1), along_y(near[1][half:], n - 1)]
    else:
        far = [along_y(w, n // 2)]
    moved = [near[0], *far, near[1]]
    return [w, *moved, swapped] + [from_other_core(v) for v in moved]


def far_first(n):
    return sorted(range(1, n), key=lambda j: -min(j, n - j))


def from_x_ring(hidden, nx):
    moved = {j: along_x(hidden, j) for j in far_first(nx)}
    return jnp.concatenate([hidden] + [moved[j] for j in range(1, nx)], axis=0)


def body(tokens, gain_first, up_first, down_first, gain_second, up_second, down_second):
    ny, nx, nz = lax.axis_size("y"), lax.axis_size("x"), lax.axis_size("z")
    count, channels = tokens.shape
    width = channels * ny * nx
    half = count // 2
    per_y = half // ny
    few = per_y // nx
    hid = 2 * up_first.shape[1]
    wide = hid + LANES
    blocks = 2 * ny

    def held(w, more=0):
        return [pltpu.VMEM((blocks, *w.shape), BF), pltpu.SemaphoreType.DMA((blocks + more,))]

    activate = call(functools.partial(activate_kernel, width=width), sds((few, hid)))
    down_out = sds((nz, per_y, LANES))

    block = pltpu.VMEM(up_first.shape, BF)
    row = pltpu.VMEM((1, channels), F32)
    up_own = call(
        up_own_kernel,
        (sds((half, wide)), sds((half, channels)), sds((per_y + 8, LANES), F32)),
        [
            pltpu.VMEM((half, channels), BF),
            row,
            row,
            pltpu.VMEM((per_y, channels), BF),
            pltpu.VMEM((nx, few, LANES), F32),
            block,
            pltpu.SemaphoreType.DMA((5,)),
        ],
        whole=0,
    )
    payload, scaled, kept = up_own(tokens, gain_first[None, :], gain_second[None, :], up_first)
    payload = call(
        up_other_kernel,
        sds((half, wide)),
        [block, pltpu.VMEM((half, hid // 2), BF), pltpu.SemaphoreType.DMA((1,))],
        whole=1,
        update=2,
    )(scaled, from_other_core(up_first), payload)
    parts = exchange(payload.reshape(ny * nx, few, wide), RA)
    kept = by_plane(kept, lambda z: z // 2)
    swapped = [from_other_core(w) for w in (down_first, up_second, down_second)]
    downs = around(down_first, swapped[0], halves=True)
    hidden = activate(parts)

    hidden = from_x_ring(hidden, nx)
    branch = call(down_kernel, down_out, held(down_first, 2), whole=1)(hidden, *downs)
    ups = around(up_second, swapped[1])
    branch = exchange(branch, "z")
    downs = around(down_second, swapped[2])
    finish_first = call(finish_first_kernel, (sds((per_y, LANES)), sds((nz, per_y + 8, LANES))))
    middle, payload = finish_first(branch, kept)
    payload = exchange(payload, "z")
    parts = call(up_second_kernel, (sds((few, wide)),) * nx, held(up_second), whole=1)(payload, *ups)
    parts = [parts[0]] + [along_x(parts[j], nx - j) for j in far_first(nx)]
    hidden = activate(*parts)
    hidden = from_x_ring(hidden, nx)
    branch = call(down_kernel, down_out, held(down_second), whole=1)(hidden, *downs)
    finished = call(finish_second_kernel, sds((per_y, LANES)))(exchange(branch, "z"), middle)
    rows = exchange(spread(by_plane(finished, lambda z: -(z // 2)), nz), "z")
    placed = pltpu.VMEM((2 * ny * nx, few, channels), F32)
    return call(assemble_kernel, sds((count, channels)), [placed])(rows, from_other_core(rows))


def solution(mesh):
    fine = Mesh(mesh.devices.reshape(4, 4, 8, 2), ("y", "x", "z", "c"))
    cb = ("z", "c")
    placed = (
        P(None, RA),
        P(RA),
        P(RA, cb),
        P(cb, RA),
        P(RA),
        P(RA, cb),
        P(cb, RA),
    )

    return jax.shard_map(body, mesh=fine, in_specs=placed, out_specs=P(None, RA), check_vma=False)
```

```python
import functools

import jax
import jax.numpy as jnp
from jax import lax
from jax.experimental import pallas as pl
from jax.experimental.pallas import tpu as pltpu
from jax.sharding import Mesh, PartitionSpec as P


RA = ("y", "x")
BF = jnp.bfloat16
F32 = jnp.float32
LANES = 128
EPS = 1e-06


def exchange(parts, axis):
    return lax.all_to_all(parts, axis, 0, 0, tiled=True)


def from_other_core(w):
    return lax.ppermute(w, "c", [(0, 1), (1, 0)])


def along_y(a, shift):
    n = lax.axis_size("y")
    return lax.ppermute(a, "y", [(i, (i + shift) % n) for i in range(n)])


def along_x(a, shift):
    n = lax.axis_size("x")
    return lax.ppermute(a, "x", [(i, (i + shift) % n) for i in range(n)])


def by_plane(a, steps):
    ny, nz = lax.axis_size("y"), lax.axis_size("z")
    perm = [(y * nz + z, (y + steps(z)) % ny * nz + z) for y in range(ny) for z in range(nz)]
    return lax.ppermute(a, ("y", "z"), perm)


def call(kernel, out, scratch=(), limit=16, whole=None, update=None, loose=0):
    vmem = pl.BlockSpec(memory_space=pltpu.VMEM)
    lies = pl.BlockSpec(memory_space=pltpu.HBM if update is None else pl.ANY)

    def run(*args):
        first = len(args) if whole is None else whole
        if update is None:
            firm = len(args) - loose
            args = [
                pltpu.with_memory_space_constraint(a, pltpu.HBM) if first <= i < firm else a
                for i, a in enumerate(args)
            ]
        return pl.pallas_call(
            kernel,
            out_shape=out,
            in_specs=[vmem] * first
            + [lies] * (len(args) - first - loose)
            + [pl.BlockSpec(memory_space=pl.ANY)] * loose,
            out_specs=jax.tree.map(lambda _: vmem if update is None else lies, out),
            scratch_shapes=list(scratch),
            input_output_aliases={} if update is None else {update: 0},
            compiler_params=pltpu.CompilerParams(vmem_limit_bytes=limit << 20),
        )(*args)

    return run


def sds(shape, dtype=BF):
    return jax.ShapeDtypeStruct(shape, dtype)


def stat_columns(sq):
    high = sq.astype(BF)
    low = (sq - high.astype(F32)).astype(BF)
    lane = lax.broadcasted_iota(jnp.int32, (sq.shape[0], LANES), 1)
    block = jnp.where(lane == 0, high.astype(F32), jnp.where(lane == 1, low.astype(F32), 0.0))
    return block.astype(BF)


def fetch(pairs, sems):
    copies = [pltpu.make_async_copy(source, held, sems.at[i]) for i, (source, held) in enumerate(pairs)]
    for copy in copies:
        copy.start()
    return copies


def up_own_kernel(tokens, gain, next_gain, own, out, scaled, kept, x, g, g2, some, some_f, w, sems):
    half, hid = x.shape[0], own.shape[1]
    rows = some.shape[0]
    nx, few, _ = some_f.shape
    y, z, c = lax.axis_index("y"), lax.axis_index("z"), lax.axis_index("c")
    first = pl.multiple_of(c * half, half)
    there = lax.rem(y + z // 2, lax.axis_size("y"))
    copies = fetch(
        (
            (gain, g),
            (tokens.at[pl.ds(first, half), :], x),
            (own, w),
            (tokens.at[pl.ds(pl.multiple_of(first + there * rows, rows), rows), :], some),
            (next_gain, g2),
        ),
        sems,
    )
    copies[0].wait()
    copies[1].wait()
    xf = x[...].astype(F32)
    out[:, 2 * hid :] = stat_columns(jnp.sum(xf * xf, axis=1, keepdims=True))
    scaled[...] = (xf * g[...]).astype(BF)
    copies[2].wait()
    out[:, :hid] = jnp.dot(scaled[...], w[...], preferred_element_type=F32).astype(BF)
    copies[3].wait()
    copies[4].wait()
    left = lax.rem(z, 2) == 0
    chosen = jnp.where(left, some[:, :LANES].astype(F32), some[:, LANES:].astype(F32))
    for i in range(nx):
        some_f[i] = chosen[i * few : (i + 1) * few]
    for j in range(nx):
        kept[j * few : (j + 1) * few, :] = some_f[lax.rem(lax.axis_index("x") + nx - j, nx)]
    chosen = jnp.where(left, g2[:, :LANES], g2[:, LANES:])
    kept[rows:, :] = jnp.broadcast_to(chosen, (8, LANES))


def up_other_kernel(scaled, other, so_far, out, w, part, sems):
    del so_far
    hid = other.shape[1]
    fetch(((other, w),), sems)[0].wait()
    part[...] = jnp.dot(scaled[...], w[...], preferred_element_type=F32).astype(BF)
    fetch(((part, out.at[:, hid : 2 * hid]),), sems)[0].wait()


def summed(parts):
    total = parts[0][...].astype(F32)
    for i in range(1, len(parts) if isinstance(parts, list) else parts.shape[0]):
        total += parts[i][...].astype(F32)
    return total


def activate_kernel(*refs, width):
    *parts, out = refs
    hid = out.shape[1]
    total = summed(parts[0] if len(parts) == 1 else parts)
    meansq = (total[:, hid : hid + 1] + total[:, hid + 1 : hid + 2]) / width
    act = jnp.maximum(total[:, :hid] * lax.rsqrt(meansq + EPS), 0.0)
    out[...] = (act * act).astype(BF)


def arriving(blocks, held, sems, order):
    n, per = held.shape[0] // 2, len(blocks) // 2
    far = n // 2
    pairs, spans = [], {}
    for side, d in order:
        mine = blocks[side * per : (side + 1) * per]
        spot = held.at[side * n + d]
        first = len(pairs)
        if d == far and per > n:
            rows = mine[far].shape[0]
            pairs += [(mine[far], spot.at[:rows]), (mine[far + 1], spot.at[rows:])]
        else:
            pairs.append((mine[d + (d > far) * (per - n)], spot))
        spans[side, d] = range(first, len(pairs))
    copies = fetch(pairs, sems)

    def ready(side, d):
        for i in spans[side, d]:
            copies[i].wait()
        return held[side * n + d]

    return ready


def down_kernel(hidden, *refs):
    *blocks, out, held, sems = refs
    n, k = held.shape[0] // 2, held.shape[1]
    ready = arriving(blocks, held, sems, [(side, d) for d in range(n) for side in range(2)])
    for d in range(n):
        acc = jnp.dot(hidden[:, :k], ready(0, d), preferred_element_type=F32)
        acc += jnp.dot(hidden[:, k:], ready(1, d), preferred_element_type=F32)
        acc = acc.astype(BF)
        out[2 * d] = acc[:, :LANES]
        out[2 * d + 1] = acc[:, LANES:]


def finish_first_kernel(parts, kept, mid, payload):
    rows = mid.shape[0]
    x = (0.5 * kept[:rows, :] + summed(parts)).astype(BF)
    gain = kept[rows:, :]
    high = gain.astype(BF).astype(F32)
    rest = gain - high
    middle = rest.astype(BF).astype(F32)
    low = rest - middle
    row = lax.broadcasted_iota(jnp.int32, gain.shape, 0)
    coded = jnp.where(row == 0, high, jnp.where(row == 1, middle, low)).astype(BF)
    mid[...] = x
    for i in range(payload.shape[0]):
        payload[i, :rows, :] = x
        payload[i, rows:, :] = coded


def up_second_kernel(x, *refs):
    *refs, held, sems = refs
    count = sems.shape[0]
    blocks, outs = refs[:count], refs[count:]
    n, depth, hid = held.shape[0] // 2, *held.shape[1:]
    ready = arriving(blocks, held, sems, [(side, d) for side in range(2) for d in range(n)])
    few = outs[0].shape[0]
    rows = few * len(outs)
    scaled, sq = [], jnp.zeros((rows, 1), F32)
    for i in range(x.shape[0]):
        xf = x[i, :rows, :].astype(F32)
        coded = x[i, rows:, :].astype(F32)
        gain = coded[0:1] + coded[1:2] + coded[2:3]
        sq += jnp.sum(xf * xf, axis=1, keepdims=True)
        scaled.append((xf * gain).astype(BF))
    scaled = jnp.concatenate(scaled, axis=1)
    for side in range(2):
        acc = jnp.zeros((rows, hid), F32)
        for d in range(n):
            acc += jnp.dot(
                scaled[:, d * depth : (d + 1) * depth], ready(side, d), preferred_element_type=F32
            )
        for j, out in enumerate(outs):
            out[:, side * hid : (side + 1) * hid] = acc[j * few : (j + 1) * few].astype(BF)
    for j, out in enumerate(outs):
        out[:, 2 * hid :] = stat_columns(sq[j * few : (j + 1) * few])


def finish_second_kernel(parts, kept, out):
    out[...] = (0.5 * kept[...].astype(F32) + summed(parts)).astype(BF)


def assemble_kernel(own, other, out, placed):
    chunks = own.shape[0]
    ny = chunks // 2
    few = placed.shape[1]
    nx = own.shape[1] // few
    x, y, c = lax.axis_index("x"), lax.axis_index("y"), lax.axis_index("c")
    for side, ref in ((c, own), (1 - c, other)):
        for i in range(chunks):
            block = ref[i].astype(F32)
            row = (side * ny + lax.rem(y + i // 2, ny)) * nx
            column = (i % 2) * LANES
            for j in range(nx):
                placed[row + lax.rem(x + nx - j, nx), :, column : column + LANES] = block[j * few : (j + 1) * few]
    out[...] = placed[...].reshape(out.shape).astype(BF)


def spread(x, peers):
    return jnp.broadcast_to(x[None], (peers, *x.shape))


def around(w, swapped, halves=False):
    n = lax.axis_size("y")
    half = w.shape[0] // 2
    near = [along_y(w, 1), along_y(w, n - 1)]
    if halves:
        far = [along_y(near[0][:half], 1), along_y(near[1][half:], n - 1)]
    else:
        far = [along_y(w, n // 2)]
    moved = [near[0], *far, near[1]]
    return [w, *moved, swapped] + [from_other_core(v) for v in moved]


def far_first(n):
    return sorted(range(1, n), key=lambda j: -min(j, n - j))


def from_x_ring(hidden, nx):
    moved = {j: along_x(hidden, j) for j in far_first(nx)}
    return jnp.concatenate([hidden] + [moved[j] for j in range(1, nx)], axis=0)


def body(tokens, gain_first, up_first, down_first, gain_second, up_second, down_second):
    ny, nx, nz = lax.axis_size("y"), lax.axis_size("x"), lax.axis_size("z")
    count, channels = tokens.shape
    width = channels * ny * nx
    half = count // 2
    per_y = half // ny
    few = per_y // nx
    hid = 2 * up_first.shape[1]
    wide = hid + LANES
    blocks = 2 * ny

    def held(w, more=0):
        return [pltpu.VMEM((blocks, *w.shape), BF), pltpu.SemaphoreType.DMA((blocks + more,))]

    activate = call(functools.partial(activate_kernel, width=width), sds((few, hid)))
    down_out = sds((nz, per_y, LANES))

    block = pltpu.VMEM(up_first.shape, BF)
    row = pltpu.VMEM((1, channels), F32)
    up_own = call(
        up_own_kernel,
        (sds((half, wide)), sds((half, channels)), sds((per_y + 8, LANES), F32)),
        [
            pltpu.VMEM((half, channels), BF),
            row,
            row,
            pltpu.VMEM((per_y, channels), BF),
            pltpu.VMEM((nx, few, LANES), F32),
            block,
            pltpu.SemaphoreType.DMA((5,)),
        ],
        whole=0,
    )
    payload, scaled, kept = up_own(tokens, gain_first[None, :], gain_second[None, :], up_first)
    payload = call(
        up_other_kernel,
        sds((half, wide)),
        [block, pltpu.VMEM((half, hid // 2), BF), pltpu.SemaphoreType.DMA((1,))],
        whole=1,
        update=2,
    )(scaled, from_other_core(up_first), payload)
    parts = exchange(payload.reshape(ny * nx, few, wide), RA)
    kept = by_plane(kept, lambda z: z // 2)
    swapped = [from_other_core(w) for w in (down_first, up_second, down_second)]
    downs = around(down_first, swapped[0], halves=True)
    hidden = activate(parts)

    hidden = from_x_ring(hidden, nx)
    branch = call(down_kernel, down_out, held(down_first, 2), whole=1, loose=ny)(hidden, *downs)
    ups = around(up_second, swapped[1])
    branch = exchange(branch, "z")
    downs = around(down_second, swapped[2])
    finish_first = call(finish_first_kernel, (sds((per_y, LANES)), sds((nz, per_y + 8, LANES))))
    middle, payload = finish_first(branch, kept)
    payload = exchange(payload, "z")
    parts = call(up_second_kernel, (sds((few, wide)),) * nx, held(up_second), whole=1, loose=ny - 1)(payload, *ups)
    parts = [parts[0]] + [along_x(parts[j], nx - j) for j in far_first(nx)]
    hidden = activate(*parts)
    hidden = from_x_ring(hidden, nx)
    branch = call(down_kernel, down_out, held(down_second), whole=1, loose=ny - 1)(hidden, *downs)
    finished = call(finish_second_kernel, sds((per_y, LANES)))(exchange(branch, "z"), middle)
    rows = exchange(spread(by_plane(finished, lambda z: -(z // 2)), nz), "z")
    placed = pltpu.VMEM((2 * ny * nx, few, channels), F32)
    return call(assemble_kernel, sds((count, channels)), [placed])(rows, from_other_core(rows))


def solution(mesh):
    fine = Mesh(mesh.devices.reshape(4, 4, 8, 2), ("y", "x", "z", "c"))
    cb = ("z", "c")
    placed = (
        P(None, RA),
        P(RA),
        P(RA, cb),
        P(cb, RA),
        P(RA),
        P(RA, cb),
        P(cb, RA),
    )

    return jax.shard_map(body, mesh=fine, in_specs=placed, out_specs=P(None, RA), check_vma=False)
```

```python
import functools

import jax
import jax.numpy as jnp
from jax import lax
from jax.experimental import pallas as pl
from jax.experimental.pallas import tpu as pltpu
from jax.sharding import Mesh, PartitionSpec as P


RA = ("y", "x")
BF = jnp.bfloat16
F32 = jnp.float32
LANES = 128
EPS = 1e-06


def exchange(parts, axis):
    return lax.all_to_all(parts, axis, 0, 0, tiled=True)


def from_other_core(w):
    return lax.ppermute(w, "c", [(0, 1), (1, 0)])


def along_y(a, shift):
    n = lax.axis_size("y")
    return lax.ppermute(a, "y", [(i, (i + shift) % n) for i in range(n)])


def along_x(a, shift):
    n = lax.axis_size("x")
    return lax.ppermute(a, "x", [(i, (i + shift) % n) for i in range(n)])


def by_plane(a, steps):
    ny, nz = lax.axis_size("y"), lax.axis_size("z")
    perm = [(y * nz + z, (y + steps(z)) % ny * nz + z) for y in range(ny) for z in range(nz)]
    return lax.ppermute(a, ("y", "z"), perm)


def call(kernel, out, scratch=(), limit=16, whole=None, update=None, loose=0):
    vmem = pl.BlockSpec(memory_space=pltpu.VMEM)
    lies = pl.BlockSpec(memory_space=pltpu.HBM if update is None else pl.ANY)

    def run(*args):
        first = len(args) if whole is None else whole
        if update is None:
            firm = len(args) - loose
            args = [
                pltpu.with_memory_space_constraint(a, pltpu.HBM) if first <= i < firm else a
                for i, a in enumerate(args)
            ]
        return pl.pallas_call(
            kernel,
            out_shape=out,
            in_specs=[vmem] * first
            + [lies] * (len(args) - first - loose)
            + [pl.BlockSpec(memory_space=pl.ANY)] * loose,
            out_specs=jax.tree.map(lambda _: vmem if update is None else lies, out),
            scratch_shapes=list(scratch),
            input_output_aliases={} if update is None else {update: 0},
            compiler_params=pltpu.CompilerParams(vmem_limit_bytes=limit << 20),
        )(*args)

    return run


def sds(shape, dtype=BF):
    return jax.ShapeDtypeStruct(shape, dtype)


def stat_columns(sq):
    high = sq.astype(BF)
    low = (sq - high.astype(F32)).astype(BF)
    lane = lax.broadcasted_iota(jnp.int32, (sq.shape[0], LANES), 1)
    block = jnp.where(lane == 0, high.astype(F32), jnp.where(lane == 1, low.astype(F32), 0.0))
    return block.astype(BF)


def fetch(pairs, sems):
    copies = [pltpu.make_async_copy(source, held, sems.at[i]) for i, (source, held) in enumerate(pairs)]
    for copy in copies:
        copy.start()
    return copies


def up_own_kernel(tokens, gain, next_gain, own, out, scaled, kept, x, g, g2, some, some_f, w, sems):
    half, hid = x.shape[0], own.shape[1]
    rows = some.shape[0]
    nx, few, _ = some_f.shape
    y, z, c = lax.axis_index("y"), lax.axis_index("z"), lax.axis_index("c")
    first = pl.multiple_of(c * half, half)
    there = lax.rem(y + z // 2, lax.axis_size("y"))
    copies = fetch(
        (
            (gain, g),
            (tokens.at[pl.ds(first, half), :], x),
            (own, w),
            (tokens.at[pl.ds(pl.multiple_of(first + there * rows, rows), rows), :], some),
            (next_gain, g2),
        ),
        sems,
    )
    copies[0].wait()
    copies[1].wait()
    xf = x[...].astype(F32)
    out[:, 2 * hid :] = stat_columns(jnp.sum(xf * xf, axis=1, keepdims=True))
    scaled[...] = (xf * g[...]).astype(BF)
    copies[2].wait()
    out[:, :hid] = jnp.dot(scaled[...], w[...], preferred_element_type=F32).astype(BF)
    copies[3].wait()
    copies[4].wait()
    left = lax.rem(z, 2) == 0
    chosen = jnp.where(left, some[:, :LANES].astype(F32), some[:, LANES:].astype(F32))
    for i in range(nx):
        some_f[i] = chosen[i * few : (i + 1) * few]
    for j in range(nx):
        kept[j * few : (j + 1) * few, :] = some_f[lax.rem(lax.axis_index("x") + nx - j, nx)]
    chosen = jnp.where(left, g2[:, :LANES], g2[:, LANES:])
    kept[rows:, :] = jnp.broadcast_to(chosen, (8, LANES))


def up_other_kernel(scaled, other, so_far, out, w, part, sems):
    del so_far
    hid = other.shape[1]
    fetch(((other, w),), sems)[0].wait()
    part[...] = jnp.dot(scaled[...], w[...], preferred_element_type=F32).astype(BF)
    fetch(((part, out.at[:, hid : 2 * hid]),), sems)[0].wait()


def summed(parts):
    total = parts[0][...].astype(F32)
    for i in range(1, len(parts) if isinstance(parts, list) else parts.shape[0]):
        total += parts[i][...].astype(F32)
    return total


def activate_kernel(*refs, width):
    *parts, out = refs
    hid = out.shape[1]
    total = summed(parts[0] if len(parts) == 1 else parts)
    meansq = (total[:, hid : hid + 1] + total[:, hid + 1 : hid + 2]) / width
    act = jnp.maximum(total[:, :hid] * lax.rsqrt(meansq + EPS), 0.0)
    out[...] = (act * act).astype(BF)


def arriving(blocks, held, sems, order):
    n, per = held.shape[0] // 2, len(blocks) // 2
    far = n // 2
    pairs, spans = [], {}
    for side, d in order:
        mine = blocks[side * per : (side + 1) * per]
        spot = held.at[side * n + d]
        first = len(pairs)
        if d == far and per > n:
            rows = mine[far].shape[0]
            pairs += [(mine[far], spot.at[:rows]), (mine[far + 1], spot.at[rows:])]
        else:
            pairs.append((mine[d + (d > far) * (per - n)], spot))
        spans[side, d] = range(first, len(pairs))
    copies = fetch(pairs, sems)

    def ready(side, d):
        for i in spans[side, d]:
            copies[i].wait()
        return held[side * n + d]

    return ready


def down_kernel(hidden, *refs):
    *blocks, out, held, sems = refs
    n, k = held.shape[0] // 2, held.shape[1]
    ready = arriving(blocks, held, sems, [(side, d) for d in range(n) for side in range(2)])
    for d in range(n):
        acc = jnp.dot(hidden[:, :k], ready(0, d), preferred_element_type=F32)
        acc += jnp.dot(hidden[:, k:], ready(1, d), preferred_element_type=F32)
        acc = acc.astype(BF)
        out[2 * d] = acc[:, :LANES]
        out[2 * d + 1] = acc[:, LANES:]


def finish_first_kernel(parts, kept, mid, payload):
    rows = mid.shape[0]
    x = (0.5 * kept[:rows, :] + summed(parts)).astype(BF)
    gain = kept[rows:, :]
    high = gain.astype(BF).astype(F32)
    rest = gain - high
    middle = rest.astype(BF).astype(F32)
    low = rest - middle
    row = lax.broadcasted_iota(jnp.int32, gain.shape, 0)
    coded = jnp.where(row == 0, high, jnp.where(row == 1, middle, low)).astype(BF)
    mid[...] = x
    for i in range(payload.shape[0]):
        payload[i, :rows, :] = x
        payload[i, rows:, :] = coded


def up_second_kernel(x, *refs):
    *refs, held, sems = refs
    count = sems.shape[0]
    blocks, outs = refs[:count], refs[count:]
    n, depth, hid = held.shape[0] // 2, *held.shape[1:]
    ready = arriving(blocks, held, sems, [(side, d) for side in range(2) for d in range(n)])
    few = outs[0].shape[0]
    rows = few * len(outs)
    scaled, sq = [], jnp.zeros((rows, 1), F32)
    for i in range(x.shape[0]):
        xf = x[i, :rows, :].astype(F32)
        coded = x[i, rows:, :].astype(F32)
        gain = coded[0:1] + coded[1:2] + coded[2:3]
        sq += jnp.sum(xf * xf, axis=1, keepdims=True)
        scaled.append((xf * gain).astype(BF))
    scaled = jnp.concatenate(scaled, axis=1)
    for side in range(2):
        acc = jnp.zeros((rows, hid), F32)
        for d in range(n):
            acc += jnp.dot(
                scaled[:, d * depth : (d + 1) * depth], ready(side, d), preferred_element_type=F32
            )
        for j, out in enumerate(outs):
            out[:, side * hid : (side + 1) * hid] = acc[j * few : (j + 1) * few].astype(BF)
    for j, out in enumerate(outs):
        out[:, 2 * hid :] = stat_columns(sq[j * few : (j + 1) * few])


def finish_second_kernel(parts, kept, out):
    out[...] = (0.5 * kept[...].astype(F32) + summed(parts)).astype(BF)


def assemble_kernel(own, other, out, placed):
    chunks = own.shape[0]
    ny = chunks // 2
    few = placed.shape[1]
    nx = own.shape[1] // few
    x, y, c = lax.axis_index("x"), lax.axis_index("y"), lax.axis_index("c")
    for side, ref in ((c, own), (1 - c, other)):
        for i in range(chunks):
            block = ref[i].astype(F32)
            row = (side * ny + lax.rem(y + i // 2, ny)) * nx
            column = (i % 2) * LANES
            for j in range(nx):
                placed[row + lax.rem(x + nx - j, nx), :, column : column + LANES] = block[j * few : (j + 1) * few]
    out[...] = placed[...].reshape(out.shape).astype(BF)


def spread(x, peers):
    return jnp.broadcast_to(x[None], (peers, *x.shape))


def around(w, swapped, halves=False):
    n = lax.axis_size("y")
    half = w.shape[0] // 2
    near = [along_y(w, 1), along_y(w, n - 1)]
    if halves:
        far = [along_y(near[0][:half], 1), along_y(near[1][half:], n - 1)]
    else:
        far = [along_y(w, n // 2)]
    moved = [near[0], *far, near[1]]
    return [w, *moved, swapped] + [from_other_core(v) for v in moved]


def far_first(n):
    return sorted(range(1, n), key=lambda j: -min(j, n - j))


def from_x_ring(hidden, nx):
    moved = {j: along_x(hidden, j) for j in far_first(nx)}
    return jnp.concatenate([hidden] + [moved[j] for j in range(1, nx)], axis=0)


def body(tokens, gain_first, up_first, down_first, gain_second, up_second, down_second):
    ny, nx, nz = lax.axis_size("y"), lax.axis_size("x"), lax.axis_size("z")
    count, channels = tokens.shape
    width = channels * ny * nx
    half = count // 2
    per_y = half // ny
    few = per_y // nx
    hid = 2 * up_first.shape[1]
    wide = hid + LANES
    blocks = 2 * ny

    def held(w, more=0):
        return [pltpu.VMEM((blocks, *w.shape), BF), pltpu.SemaphoreType.DMA((blocks + more,))]

    activate = call(functools.partial(activate_kernel, width=width), sds((few, hid)))
    down_out = sds((nz, per_y, LANES))

    block = pltpu.VMEM(up_first.shape, BF)
    row = pltpu.VMEM((1, channels), F32)
    up_own = call(
        up_own_kernel,
        (sds((half, wide)), sds((half, channels)), sds((per_y + 8, LANES), F32)),
        [
            pltpu.VMEM((half, channels), BF),
            row,
            row,
            pltpu.VMEM((per_y, channels), BF),
            pltpu.VMEM((nx, few, LANES), F32),
            block,
            pltpu.SemaphoreType.DMA((5,)),
        ],
        whole=0,
    )
    payload, scaled, kept = up_own(tokens, gain_first[None, :], gain_second[None, :], up_first)
    payload = call(
        up_other_kernel,
        sds((half, wide)),
        [block, pltpu.VMEM((half, hid // 2), BF), pltpu.SemaphoreType.DMA((1,))],
        whole=1,
        update=2,
    )(scaled, from_other_core(up_first), payload)
    parts = exchange(payload.reshape(ny * nx, few, wide), RA)
    kept = by_plane(kept, lambda z: z // 2)
    swapped = [from_other_core(w) for w in (down_first, up_second, down_second)]
    downs = around(down_first, swapped[0], halves=True)
    hidden = activate(parts)

    hidden = from_x_ring(hidden, nx)
    branch = call(down_kernel, down_out, held(down_first, 2), whole=1, loose=2 * ny + 1)(hidden, *downs)
    ups = around(up_second, swapped[1])
    branch = exchange(branch, "z")
    downs = around(down_second, swapped[2])
    finish_first = call(finish_first_kernel, (sds((per_y, LANES)), sds((nz, per_y + 8, LANES))))
    middle, payload = finish_first(branch, kept)
    payload = exchange(payload, "z")
    parts = call(up_second_kernel, (sds((few, wide)),) * nx, held(up_second), whole=1, loose=2 * ny - 1)(payload, *ups)
    parts = [parts[0]] + [along_x(parts[j], nx - j) for j in far_first(nx)]
    hidden = activate(*parts)
    hidden = from_x_ring(hidden, nx)
    branch = call(down_kernel, down_out, held(down_second), whole=1, loose=2 * ny - 1)(hidden, *downs)
    finished = call(finish_second_kernel, sds((per_y, LANES)))(exchange(branch, "z"), middle)
    rows = exchange(spread(by_plane(finished, lambda z: -(z // 2)), nz), "z")
    placed = pltpu.VMEM((2 * ny * nx, few, channels), F32)
    return call(assemble_kernel, sds((count, channels)), [placed])(rows, from_other_core(rows))


def solution(mesh):
    fine = Mesh(mesh.devices.reshape(4, 4, 8, 2), ("y", "x", "z", "c"))
    cb = ("z", "c")
    placed = (
        P(None, RA),
        P(RA),
        P(RA, cb),
        P(cb, RA),
        P(RA),
        P(RA, cb),
        P(cb, RA),
    )

    return jax.shard_map(body, mesh=fine, in_specs=placed, out_specs=P(None, RA), check_vma=False)
```
